32 devices in a mesh: sp: 16 (over z, y, x), tp: 2 (over core).
Axes of the slice: x: 2, y: 2, z: 4, core: 2. Of those that a mesh axis runs over, the one named last changes fastest.
Arguments:
- tokens: bfloat16 [3072, 4096], P('sp'), may hold values from -6 to 6
- norm_gain: float32 [4096], replicated, may hold values from 0.1 to 1.9
- conv_value: bfloat16 [4096, 2048], P('sp', 'tp'), may hold values from -0.09375 to 0.09375
- conv_gate: bfloat16 [4096, 2048], P('sp', 'tp'), may hold values from -0.09375 to 0.09375
- state_feed: bfloat16 [4096, 2048], P('sp', 'tp'), may hold values from -0.09375 to 0.09375
- conv_taps: float32 [31, 2048], P(None, 'tp'), may hold values from -1 to 1
- chan_gain: float32 [2048], replicated, may hold values from 0.1 to 1.9
- chan_shift: float32 [2048], replicated, may hold values from -3 to 3
- conv_project: bfloat16 [2048, 4096], P('sp', 'tp'), may hold values from -0.125 to 0.125
- decay_rate: float32 [128, 64], P('tp'), may hold values from 0.1 to 3
- frequency: float32 [128, 64], P('tp'), may hold values from 0.1 to 3
- input_real: float32 [128, 64, 16], P('tp'), may hold values from -0.0390625 to 0.0390625
- input_imag: float32 [128, 64, 16], P('tp'), may hold values from -0.0390625 to 0.0390625
- output_real: float32 [128, 16, 64], P('tp'), may hold values from -0.5 to 0.5
- output_imag: float32 [128, 16, 64], P('tp'), may hold values from -0.5 to 0.5
- skip_gain: float32 [2048], P('tp'), may hold values from -3 to 3
- state_value: bfloat16 [2048, 4096], P('sp', 'tp'), may hold values from -0.125 to 0.125
- state_gate: bfloat16 [2048, 4096], P('sp', 'tp'), may hold values from -0.125 to 0.125
- initial_state: float32 [2, 128, 64], P(None, 'tp'), may hold values from -5 to 5
Outputs:
- mixer_out: bfloat16 [3072, 4096], P('sp', 'tp')
- final_state: float32 [2, 128, 64], P(None, 'tp')
The draws below stay inside these ranges and needn't reach their ends.
All inputs are finite; a program needn't handle non-finite values.
Results may differ from the reference program's by a relative error of at most 0.0085.
Values may be sent and summed in bfloat16 or wider, within the bound.
A program may use at most 128 MiB of HBM per device.

```python
import math
import jax
import jax.numpy as jnp
from jax import lax

D = 4096
CH = 2048
GROUP = 16
STATE = 64
KERNEL = 31
TOKENS = 3072
GROUPS = 128


def steps_of(rng, extent, split, low, largest):
    def one(dim, shards_of):
        steps = jax.random.uniform(jax.random.fold_in(jax.random.fold_in(rng, 6), dim), (shards_of,), jnp.float32, low / len(split), largest / len(split))
        return jnp.repeat(jnp.exp(steps), extent[dim] // shards_of).reshape((-1,) + (1,) * (len(extent) - dim - 1))

    factor_of = one(*split[0])
    for cut in split[1:]:
        factor_of = factor_of * one(*cut)
    return factor_of


def bell_draw(rng, extent, scale, bound, split=(), held_as=jnp.bfloat16):
    result = jax.random.normal(rng, extent, jnp.float32) * scale
    if len(split) > 0:
        result = steps_of(rng, extent, split, -0.22, 0.18) * result
    return jnp.clip(result, min=-bound, max=bound).astype(held_as)


def setup_inputs(seed: int = 0) -> dict:
    key_of = jax.random.split(jax.random.key(seed), 20)
    tokens = bell_draw(key_of[0], (TOKENS, D), 1.0, 6.0, ((0, 16),))
    norm_gain = jnp.clip(1.0 + 0.18 * jax.random.normal(key_of[1], (D,), jnp.float32), 0.1, 1.9)
    conv_value = bell_draw(key_of[2], (D, CH), D ** -0.5, 0.09375, ((0, 16), (1, 2)))
    conv_gate = bell_draw(key_of[3], (D, CH), D ** -0.5, 0.09375, ((0, 16), (1, 2)))
    state_feed = bell_draw(key_of[4], (D, CH), D ** -0.5, 0.09375, ((0, 16), (1, 2)))
    conv_taps = bell_draw(key_of[5], (KERNEL, CH), KERNEL ** -0.5, 1.0, ((1, 2),), jnp.float32)
    chan_gain = jnp.clip(1.0 + 0.18 * jax.random.normal(key_of[6], (CH,), jnp.float32), 0.1, 1.9)
    chan_shift = bell_draw(key_of[7], (CH,), 0.5, 3.0, (), jnp.float32)
    conv_project = bell_draw(key_of[8], (CH, D), CH ** -0.5, 0.125, ((0, 16), (1, 2)))
    decay_rate = jnp.clip(jnp.exp(math.log(3.0) - 3.4011974 * jax.random.uniform(key_of[9], (GROUPS, STATE), jnp.float32) ** steps_of(key_of[9], (GROUPS, STATE), ((0, 2),), -0.2, 0.2)), 0.1, 3.0)
    frequency = jnp.clip(0.1 + 2.9 * jax.random.uniform(key_of[10], (GROUPS, STATE), jnp.float32) ** steps_of(key_of[10], (GROUPS, STATE), ((0, 2),), -0.2, 0.2), 0.1, 3.0)
    input_real = bell_draw(key_of[11], (GROUPS, STATE, GROUP), (8 * TOKENS) ** -0.5, 0.0390625, ((0, 2),), jnp.float32)
    input_imag = bell_draw(key_of[12], (GROUPS, STATE, GROUP), (8 * TOKENS) ** -0.5, 0.0390625, ((0, 2),), jnp.float32)
    output_real = bell_draw(key_of[13], (GROUPS, GROUP, STATE), (2 * STATE) ** -0.5, 0.5, ((0, 2),), jnp.float32)
    output_imag = bell_draw(key_of[14], (GROUPS, GROUP, STATE), (2 * STATE) ** -0.5, 0.5, ((0, 2),), jnp.float32)
    skip_gain = bell_draw(key_of[15], (CH,), 0.5, 3.0, ((0, 2),), jnp.float32)
    state_value = bell_draw(key_of[16], (CH, D), CH ** -0.5, 0.125, ((0, 16), (1, 2)))
    state_gate = bell_draw(key_of[17], (CH, D), CH ** -0.5, 0.125, ((0, 16), (1, 2)))
    initial_state = bell_draw(key_of[18], (2, GROUPS, STATE), 1.0, 5.0, ((1, 2),), jnp.float32)
    return dict(tokens=tokens, norm_gain=norm_gain, conv_value=conv_value, conv_gate=conv_gate, state_feed=state_feed, conv_taps=conv_taps, chan_gain=chan_gain, chan_shift=chan_shift, conv_project=conv_project, decay_rate=decay_rate, frequency=frequency, input_real=input_real, input_imag=input_imag, output_real=output_real, output_imag=output_imag, skip_gain=skip_gain, state_value=state_value, state_gate=state_gate, initial_state=initial_state)


def reference(tokens, norm_gain, conv_value, conv_gate, state_feed, conv_taps, chan_gain, chan_shift, conv_project, decay_rate, frequency, input_real, input_imag, output_real, output_imag, skip_gain, state_value, state_gate, initial_state):
    highest = lax.Precision.HIGHEST
    floats = tokens.astype(jnp.float32)
    normed = (floats * lax.rsqrt(lax.optimization_barrier(jnp.mean(floats * floats, axis=1, keepdims=True)) + 1e-06) * norm_gain).astype(jnp.bfloat16)
    value_in = jnp.dot(normed, conv_value, preferred_element_type=jnp.float32)
    gate_in = jnp.dot(normed, conv_gate, preferred_element_type=jnp.float32)
    gated_linear = (value_in * jax.nn.sigmoid(gate_in)).astype(jnp.bfloat16)
    kernel = conv_taps.shape[0]
    length = tokens.shape[0]
    padded = jnp.pad(gated_linear.astype(jnp.float32), ((kernel - 1, 0), (0, 0)))
    conv_sum = jnp.zeros(gated_linear.shape, jnp.float32)
    for offset in range(kernel):
        conv_sum = conv_sum + conv_taps[offset] * padded[offset:offset + length]
    conv_out = conv_sum.astype(jnp.bfloat16)
    conv_full = conv_out.astype(jnp.float32)
    row_mean = lax.optimization_barrier(jnp.mean(conv_full, axis=1, keepdims=True))
    centred = conv_full - row_mean
    variance = lax.optimization_barrier(jnp.mean(centred * centred, axis=1, keepdims=True))
    conv_act = jax.nn.silu(centred * lax.rsqrt(variance + 1e-05) * chan_gain + chan_shift).astype(jnp.bfloat16)
    conv_branch = jnp.dot(conv_act, conv_project, preferred_element_type=jnp.float32)
    state_drive = jnp.dot(normed, state_feed, preferred_element_type=jnp.float32).astype(jnp.bfloat16)
    groups, state_size, group_size = input_real.shape
    rate_real = -decay_rate / TOKENS
    magnitude = jnp.exp(rate_real)
    step_real = magnitude * jnp.cos(frequency)
    step_imag = magnitude * jnp.sin(frequency)
    modulus = rate_real * rate_real + frequency * frequency
    lift_real = step_real - 1.0
    factor_real = (lift_real * rate_real + step_imag * frequency) / modulus
    factor_imag = (step_imag * rate_real - lift_real * frequency) / modulus
    drive_real = factor_real[..., None] * input_real - factor_imag[..., None] * input_imag
    drive_imag = factor_real[..., None] * input_imag + factor_imag[..., None] * input_real
    grouped = state_drive.astype(jnp.float32).reshape(length, groups, group_size)

    def advance(carried, token_in):
        prior_real, prior_imag = carried
        pushed_real = jnp.einsum('gph,gh->gp', drive_real, token_in, precision=highest)
        pushed_imag = jnp.einsum('gph,gh->gp', drive_imag, token_in, precision=highest)
        next_real = step_real * prior_real - step_imag * prior_imag + pushed_real
        next_imag = step_real * prior_imag + step_imag * prior_real + pushed_imag
        emitted = jnp.einsum('ghp,gp->gh', output_real, next_real, precision=highest) - jnp.einsum('ghp,gp->gh', output_imag, next_imag, precision=highest)
        return ((next_real, next_imag), emitted)
    (last_real, last_imag), responses = lax.scan(advance, (initial_state[0], initial_state[1]), grouped)
    response = responses.reshape(length, groups * group_size) + skip_gain * state_drive.astype(jnp.float32)
    activated = jax.nn.gelu(response).astype(jnp.bfloat16)
    state_values = jnp.dot(activated, state_value, preferred_element_type=jnp.float32)
    state_gates = jnp.dot(activated, state_gate, preferred_element_type=jnp.float32)
    mixer_out = (conv_branch + state_values * jax.nn.sigmoid(state_gates)).astype(jnp.bfloat16)
    final_state = jnp.stack([last_real, last_imag])
    return (mixer_out, final_state)
```

```python
import jax
import jax.numpy as jnp
from jax import lax
from jax.sharding import PartitionSpec as P


def passed_along(value, axis, steps):
    count = lax.axis_size(axis)
    leading, last = (max(0, -steps), min(count, count - steps))
    return lax.ppermute(value, axis, [(source, source + steps) for source in range(leading, last)])


def rotate(first_real, first_imag, second_real, second_imag):
    return (
        first_real * second_real - first_imag * second_imag,
        first_real * second_imag + first_imag * second_real,
    )


def power_table(base_real, base_imag, exponent, largest):
    result_real = jnp.ones((exponent.shape[0], base_real.shape[0]), jnp.float32)
    result_imag = jnp.zeros((exponent.shape[0], base_real.shape[0]), jnp.float32)
    square_real, square_imag = (base_real, base_imag)
    for place in range(max(largest, 1).bit_length()):
        chosen = (exponent >> place & 1 == 1)[:, None]
        next_real, next_imag = rotate(result_real, result_imag, square_real, square_imag)
        result_real = jnp.where(chosen, next_real, result_real)
        result_imag = jnp.where(chosen, next_imag, result_imag)
        square_real, square_imag = rotate(square_real, square_imag, square_real, square_imag)
    return (result_real, result_imag)


def local(
    tokens,
    norm_gain,
    conv_value,
    conv_gate,
    state_feed,
    conv_taps,
    chan_gain,
    chan_shift,
    conv_project,
    decay_rate,
    frequency,
    input_real,
    input_imag,
    output_real,
    output_imag,
    skip_gain,
    state_value,
    state_gate,
    initial_state,
):
    highest = lax.Precision.HIGHEST
    floats = tokens.astype(jnp.float32)
    normed = (
        floats * lax.rsqrt(jnp.mean(floats * floats, axis=1, keepdims=True) + 1e-06) * norm_gain
    ).astype(jnp.bfloat16)
    length = tokens.shape[0]
    width = conv_value.shape[1]
    in_block = jnp.concatenate([conv_value, conv_gate, state_feed], axis=1)
    projected = jnp.dot(
        normed,
        lax.all_gather(in_block, "sp", axis=0, tiled=True),
        preferred_element_type=jnp.float32,
    )
    gated_linear = (projected[:, :width] * jax.nn.sigmoid(projected[:, width : 2 * width])).astype(
        jnp.bfloat16
    )
    state_drive = projected[:, 2 * width :].astype(jnp.bfloat16)
    kernel = conv_taps.shape[0]
    before = passed_along(gated_linear[length - (kernel - 1) :], "sp", 1)
    padded = jnp.concatenate([before, gated_linear], axis=0).astype(jnp.float32)
    conv_sum = jnp.zeros((length, width), jnp.float32)
    for offset in range(kernel):
        conv_sum = conv_sum + conv_taps[offset] * padded[offset : offset + length]
    conv_out = conv_sum.astype(jnp.bfloat16)
    seq_devices = lax.axis_size("sp")
    total_tokens = length * seq_devices
    groups, state_size, group_size = input_real.shape
    flat = groups * state_size
    rate_real = -decay_rate / total_tokens
    magnitude = jnp.exp(rate_real)
    step_real = magnitude * jnp.cos(frequency)
    step_imag = magnitude * jnp.sin(frequency)
    modulus = rate_real * rate_real + frequency * frequency
    lift_real = step_real - 1.0
    factor_real = (lift_real * rate_real + step_imag * frequency) / modulus
    factor_imag = (step_imag * rate_real - lift_real * frequency) / modulus
    drive_real = factor_real[..., None] * input_real - factor_imag[..., None] * input_imag
    drive_imag = factor_real[..., None] * input_imag + factor_imag[..., None] * input_real
    grouped = state_drive.astype(jnp.float32).reshape(length, groups, group_size)
    pushed_real = jnp.einsum("gph,tgh->tgp", drive_real, grouped, precision=highest).reshape(
        length, flat
    )
    pushed_imag = jnp.einsum("gph,tgh->tgp", drive_imag, grouped, precision=highest).reshape(
        length, flat
    )
    base_real = step_real.reshape(flat)
    base_imag = step_imag.reshape(flat)
    square_size = base_real * base_real + base_imag * base_imag
    back_real = base_real / square_size
    back_imag = -base_imag / square_size
    positions = lax.iota(jnp.int32, length)
    counted = positions + 1
    power_real, power_imag = power_table(base_real, base_imag, counted, length)
    undo_real, undo_imag = power_table(back_real, back_imag, counted, length)
    scaled_real, scaled_imag = rotate(undo_real, undo_imag, pushed_real, pushed_imag)
    lower = (positions[:, None] >= positions[None, :]).astype(jnp.float32)
    summed_real = jnp.dot(lower, scaled_real, precision=highest)
    summed_imag = jnp.dot(lower, scaled_imag, precision=highest)
    local_real, local_imag = rotate(power_real, power_imag, summed_real, summed_imag)
    span_real, span_imag = (power_real[-1], power_imag[-1])
    last_real, last_imag = (local_real[-1], local_imag[-1])
    start_real = initial_state[0].reshape(flat)
    start_imag = initial_state[1].reshape(flat)
    finals = lax.all_gather(jnp.stack([last_real, last_imag])[None], "sp", axis=0, tiled=True)
    position = lax.axis_index("sp")
    device_ids = lax.iota(jnp.int32, seq_devices)
    lag = jnp.maximum(position - 1 - device_ids, 0)
    weight_real, weight_imag = power_table(span_real, span_imag, lag, seq_devices)
    before_mask = (device_ids < position).astype(jnp.float32)[:, None]
    moved_real, moved_imag = rotate(weight_real, weight_imag, finals[:, 0], finals[:, 1])
    lead_real, lead_imag = power_table(
        span_real, span_imag, jnp.stack([position, jnp.int32(seq_devices)]), seq_devices
    )
    opening_real, opening_imag = rotate(lead_real[0], lead_imag[0], start_real, start_imag)
    entry_real = opening_real + jnp.sum(moved_real * before_mask, axis=0)
    entry_imag = opening_imag + jnp.sum(moved_imag * before_mask, axis=0)
    tail_real, tail_imag = power_table(
        span_real, span_imag, seq_devices - 1 - device_ids, seq_devices
    )
    carried_real, carried_imag = rotate(tail_real, tail_imag, finals[:, 0], finals[:, 1])
    closing_real, closing_imag = rotate(lead_real[1], lead_imag[1], start_real, start_imag)
    final_real = closing_real + jnp.sum(carried_real, axis=0)
    final_imag = closing_imag + jnp.sum(carried_imag, axis=0)
    final_state = jnp.stack([final_real, final_imag]).reshape(2, groups, state_size)
    state_real = (power_real * entry_real - power_imag * entry_imag + local_real).reshape(
        length, groups, state_size
    )
    state_imag = (power_real * entry_imag + power_imag * entry_real + local_imag).reshape(
        length, groups, state_size
    )
    response = jnp.einsum("ghp,tgp->tgh", output_real, state_real, precision=highest) - jnp.einsum(
        "ghp,tgp->tgh", output_imag, state_imag, precision=highest
    )
    response = response.reshape(length, groups * group_size) + skip_gain * state_drive.astype(
        jnp.float32
    )
    activated = jax.nn.gelu(response).astype(jnp.bfloat16)
    conv_rows, activated_rows = (
        lax.all_gather(conv_out, "tp", axis=1, tiled=True),
        lax.all_gather(activated, "tp", axis=1, tiled=True),
    )
    conv_full = conv_rows.astype(jnp.float32)
    row_mean = jnp.mean(conv_full, axis=1, keepdims=True)
    centred = conv_full - row_mean
    variance = jnp.mean(centred * centred, axis=1, keepdims=True)
    conv_act = jax.nn.silu(centred * lax.rsqrt(variance + 1e-05) * chan_gain + chan_shift).astype(
        jnp.bfloat16
    )
    columns = conv_project.shape[1]
    out_block = jnp.concatenate([conv_project, state_value, state_gate], axis=1)
    piece = lax.all_gather(out_block, "sp", axis=0, tiled=True)
    conv_branch = jnp.dot(conv_act, piece[:, :columns], preferred_element_type=jnp.float32)
    state_both = jnp.dot(activated_rows, piece[:, columns:], preferred_element_type=jnp.float32)
    mixer_out = (
        conv_branch + state_both[:, :columns] * jax.nn.sigmoid(state_both[:, columns:])
    ).astype(jnp.bfloat16)
    return (mixer_out, final_state)


def power_stack(base_real, base_imag, count):
    real, imag = (base_real[None], base_imag[None])
    while real.shape[0] < count:
        next_real, next_imag = rotate(real, imag, real[-1:], imag[-1:])
        real = jnp.concatenate([real, next_real], axis=0)
        imag = jnp.concatenate([imag, next_imag], axis=0)
    return (real[:count], imag[:count])


def block_diagonal(blocks):
    groups = blocks.shape[1]
    return blocks[:, :, :, None, :] * jnp.eye(groups, dtype=blocks.dtype)[None, :, None, :, None]


def chunk_matrices(decay_rate, frequency, input_real, input_imag, output_real, output_imag, total, chunk):
    highest = lax.Precision.HIGHEST
    groups, states, width = input_real.shape
    rate_real = -decay_rate / total
    magnitude = jnp.exp(rate_real)
    step_real = magnitude * jnp.cos(frequency)
    step_imag = magnitude * jnp.sin(frequency)
    modulus = rate_real * rate_real + frequency * frequency
    lift_real = step_real - 1.0
    factor_real = (lift_real * rate_real + step_imag * frequency) / modulus
    factor_imag = (step_imag * rate_real - lift_real * frequency) / modulus
    drive_real = factor_real[..., None] * input_real - factor_imag[..., None] * input_imag
    drive_imag = factor_real[..., None] * input_imag + factor_imag[..., None] * input_real
    power_real, power_imag = power_stack(step_real, step_imag, chunk)
    whole_real = jnp.concatenate([jnp.ones_like(step_real)[None], power_real], axis=0)
    whole_imag = jnp.concatenate([jnp.zeros_like(step_imag)[None], power_imag], axis=0)
    back_real = whole_real[:chunk][::-1, :, :, None]
    back_imag = whole_imag[:chunk][::-1, :, :, None]
    push_real, push_imag = rotate(back_real, back_imag, drive_real[None], drive_imag[None])
    push = [
        block_diagonal(value.transpose(0, 1, 3, 2)).reshape(chunk * groups * width, groups * states)
        for value in (push_real, push_imag)
    ]
    push = jnp.concatenate(push, axis=1)
    out_real, out_imag = rotate(
        output_real[None], output_imag[None], whole_real[:, :, None, :], whole_imag[:, :, None, :]
    )
    emit = [
        block_diagonal(value.transpose(1, 3, 0, 2).reshape(1, groups, states, chunk * width))
        for value in (out_real[1:], -out_imag[1:])
    ]
    emit = [
        value.reshape(groups, states, groups, chunk, width)
        .transpose(0, 1, 3, 2, 4)
        .reshape(groups * states, chunk * groups * width)
        for value in emit
    ]
    emit = jnp.concatenate(emit, axis=0)
    response = jnp.einsum(
        "dghp,gpi->dgih", out_real[:chunk], drive_real, precision=highest
    ) - jnp.einsum("dghp,gpi->dgih", out_imag[:chunk], drive_imag, precision=highest)
    spread = block_diagonal(response).reshape(chunk, groups * width, groups * width)
    spread = spread.transpose(1, 0, 2).reshape(groups * width, chunk * groups * width)
    padded = jnp.concatenate([jnp.zeros_like(spread), spread], axis=1)
    span = groups * width
    full = chunk * span
    inside = jnp.concatenate(
        [padded[:, full - place * span : 2 * full - place * span] for place in range(chunk)], axis=0
    )
    return (power_real[-1].reshape(-1), power_imag[-1].reshape(-1), push, emit, inside)


def recurrence(feed, skip_gain, start, matrices, chunk):
    highest = lax.Precision.HIGHEST
    span_real, span_imag, push, emit, inside = matrices
    length, width = feed.shape
    count = length // chunk
    rows = feed.reshape(count, chunk * width).astype(jnp.float32)
    pushed = jnp.dot(rows, push, precision=highest)
    flat = span_real.shape[0]
    first_real, first_imag = rotate(span_real, span_imag, start[0], start[1])
    head = jnp.concatenate([first_real, first_imag])[None]
    pushed = jnp.concatenate([pushed[:1] + head, pushed[1:]], axis=0)
    real, imag = (pushed[:, :flat], pushed[:, flat:])
    shift = 1
    while shift < count:
        moved_real = jnp.pad(real[:-shift], ((shift, 0), (0, 0)))
        moved_imag = jnp.pad(imag[:-shift], ((shift, 0), (0, 0)))
        add_real, add_imag = rotate(span_real, span_imag, moved_real, moved_imag)
        real, imag = (real + add_real, imag + add_imag)
        span_real, span_imag = rotate(span_real, span_imag, span_real, span_imag)
        shift *= 2
    entry_real = jnp.concatenate([start[0][None], real[:-1]], axis=0)
    entry_imag = jnp.concatenate([start[1][None], imag[:-1]], axis=0)
    entry = jnp.concatenate([entry_real, entry_imag], axis=1)
    response = jnp.dot(rows, inside, precision=highest) + jnp.dot(entry, emit, precision=highest)
    response = response + jnp.tile(skip_gain, chunk) * rows
    activated = jax.nn.gelu(response).astype(jnp.bfloat16).reshape(length, width)
    return (activated, jnp.stack([real[-1], imag[-1]]))


def channel_local(
    tokens,
    norm_gain,
    conv_value,
    conv_gate,
    state_feed,
    conv_taps,
    chan_gain,
    chan_shift,
    conv_project,
    decay_rate,
    frequency,
    input_real,
    input_imag,
    output_real,
    output_imag,
    skip_gain,
    state_value,
    state_gate,
    initial_state,
):
    seq = ("outer", "inner")
    devices = lax.axis_size("outer") * lax.axis_size("inner")
    inner = lax.axis_size("inner")
    position = lax.axis_index("outer") * inner + lax.axis_index("inner")
    core = lax.axis_index("tp")
    swap = [(0, 1), (1, 0)]
    local_length, model = tokens.shape
    total = local_length * devices
    half = model // 2
    floats = tokens.astype(jnp.float32)
    normed = (
        floats * lax.rsqrt(jnp.mean(floats * floats, axis=1, keepdims=True) + 1e-06) * norm_gain
    ).astype(jnp.bfloat16)
    own_half = lax.dynamic_slice_in_dim(normed, core * half, half, axis=1)
    all_half = lax.all_gather(own_half, seq, axis=0, tiled=True)
    rows, wide = conv_value.shape
    share = wide // devices
    in_block = jnp.stack([conv_value, conv_gate, state_feed], axis=1)
    in_block = in_block.reshape(rows, 3, devices, share).transpose(2, 0, 1, 3)
    in_block = in_block.reshape(devices, rows, 3 * share)
    in_block = lax.all_to_all(in_block, seq, 0, 0, tiled=True).reshape(model, 3 * share)
    kept = lax.dynamic_slice_in_dim(in_block, core * half, half, axis=0)
    given = lax.dynamic_slice_in_dim(in_block, (1 - core) * half, half, axis=0)
    taken = lax.ppermute(given, "tp", swap)
    out_rows, columns = conv_project.shape
    piece = columns // inner
    out_block = jnp.stack([conv_project, state_value, state_gate], axis=1)
    out_block = out_block.reshape(out_rows, 3, inner, piece).transpose(2, 0, 1, 3)
    out_block = out_block.reshape(inner, out_rows, 3 * piece)
    out_block = lax.all_to_all(out_block, "inner", 0, 0, tiled=True)
    out_block = lax.all_gather(
        out_block.reshape(inner * out_rows, 3 * piece), "outer", axis=0, tiled=True
    )
    groups = decay_rate.shape[0] // devices
    chunk = 16

    def own(value, axis=0, size=groups):
        return lax.dynamic_slice_in_dim(value, position * size, size, axis=axis)

    matrices = chunk_matrices(
        own(decay_rate),
        own(frequency),
        own(input_real),
        own(input_imag),
        own(output_real),
        own(output_imag),
        total,
        chunk,
    )
    other = lax.ppermute(jnp.dot(all_half, taken, preferred_element_type=jnp.float32), "tp", swap)
    projected = jnp.dot(all_half, kept, preferred_element_type=jnp.float32) + other
    gated = (projected[:, :share] * jax.nn.sigmoid(projected[:, share : 2 * share])).astype(
        jnp.bfloat16
    )
    feed = projected[:, 2 * share :].astype(jnp.bfloat16)
    kernel = conv_taps.shape[0]
    taps = own(conv_taps, 1, share)
    padded = jnp.pad(gated, ((kernel - 1, 0), (0, 0))).astype(jnp.float32)
    conv_sum = jnp.zeros((total, share), jnp.float32)
    for offset in range(kernel):
        conv_sum = conv_sum + taps[offset] * padded[offset : offset + total]
    conv_out = conv_sum.astype(jnp.bfloat16)
    start = own(initial_state, 1).reshape(2, -1)
    activated, last = recurrence(feed, own(skip_gain, 0, share), start, matrices, chunk)
    states = initial_state.shape[2]
    final_state = lax.all_gather(last.reshape(2, groups, states), seq, axis=1, tiled=True)
    mixed = jnp.concatenate([conv_out, activated], axis=1).reshape(devices, local_length, 2 * share)
    mixed = lax.all_to_all(mixed, seq, 0, 0, tiled=True).transpose(1, 0, 2)
    conv_full = mixed[:, :, :share].reshape(local_length, wide).astype(jnp.float32)
    active = mixed[:, :, share:].reshape(local_length, wide)
    own_mean = jnp.mean(conv_full, axis=1, keepdims=True)
    deviation = conv_full - own_mean
    own_spread = jnp.mean(deviation * deviation, axis=1, keepdims=True)
    peer = lax.ppermute(jnp.concatenate([own_mean, own_spread], axis=1), "tp", swap)
    row_mean = 0.5 * (own_mean + peer[:, :1])
    gap = 0.5 * (own_mean - peer[:, :1])
    variance = 0.5 * (own_spread + peer[:, 1:]) + gap * gap
    gain = lax.dynamic_slice_in_dim(chan_gain, core * wide, wide, axis=0)
    bias = lax.dynamic_slice_in_dim(chan_shift, core * wide, wide, axis=0)
    conv_act = jax.nn.silu(
        (conv_full - row_mean) * lax.rsqrt(variance + 1e-05) * gain + bias
    ).astype(jnp.bfloat16)
    both = jnp.stack([conv_act, active], axis=0)
    both = lax.all_gather(both, "inner", axis=1, tiled=True)
    both = lax.all_gather(both, "tp", axis=2, tiled=True)
    conv_branch = jnp.dot(both[0], out_block[:, :piece], preferred_element_type=jnp.float32)
    state_both = jnp.dot(both[1], out_block[:, piece:], preferred_element_type=jnp.float32)
    mixer = (conv_branch + state_both[:, :piece] * jax.nn.sigmoid(state_both[:, piece:])).astype(
        jnp.bfloat16
    )
    mixer = mixer.reshape(inner, local_length, piece)
    mixer = lax.all_to_all(mixer, "inner", 0, 0, tiled=True)
    mixer_out = mixer.transpose(1, 0, 2).reshape(local_length, columns)
    return (mixer_out, final_state)


def specs_of(seq):
    in_specs = (
        P(seq, None),
        P(),
        P(seq, "tp"),
        P(seq, "tp"),
        P(seq, "tp"),
        P(None, "tp"),
        P(),
        P(),
        P(seq, "tp"),
        P("tp", None),
        P("tp", None),
        P("tp", None, None),
        P("tp", None, None),
        P("tp", None, None),
        P("tp", None, None),
        P("tp"),
        P(seq, "tp"),
        P(seq, "tp"),
        P(None, "tp", None),
    )
    return (in_specs, (P(seq, "tp"), P(None, "tp", None)))


def solution(mesh):
    seq_devices, cores = (mesh.shape["sp"], mesh.shape["tp"])
    fine = jax.sharding.Mesh(
        mesh.devices.reshape(seq_devices // 4, 4, cores), ("outer", "inner", "tp")
    )

    def run(*args):
        groups = args[9].shape[0]
        if cores == 2 and groups % (cores * seq_devices) == 0:
            in_specs, out_specs = specs_of(("outer", "inner"))
            body = jax.shard_map(
                channel_local, mesh=fine, in_specs=in_specs, out_specs=out_specs, check_vma=False
            )
        else:
            in_specs, out_specs = specs_of("sp")
            body = jax.shard_map(
                local, mesh=mesh, in_specs=in_specs, out_specs=out_specs, check_vma=False
            )
        return body(*args)

    return run
```

```python
import functools
import jax
import jax.numpy as jnp
from jax import lax
from jax.experimental import pallas as pl
from jax.experimental.pallas import tpu as pltpu
from jax.sharding import PartitionSpec as P


def passed_along(value, axis, steps):
    count = lax.axis_size(axis)
    leading, last = (max(0, -steps), min(count, count - steps))
    return lax.ppermute(value, axis, [(source, source + steps) for source in range(leading, last)])


def rotate(first_real, first_imag, second_real, second_imag):
    return (
        first_real * second_real - first_imag * second_imag,
        first_real * second_imag + first_imag * second_real,
    )


def power_table(base_real, base_imag, exponent, largest):
    result_real = jnp.ones((exponent.shape[0], base_real.shape[0]), jnp.float32)
    result_imag = jnp.zeros((exponent.shape[0], base_real.shape[0]), jnp.float32)
    square_real, square_imag = (base_real, base_imag)
    for place in range(max(largest, 1).bit_length()):
        chosen = (exponent >> place & 1 == 1)[:, None]
        next_real, next_imag = rotate(result_real, result_imag, square_real, square_imag)
        result_real = jnp.where(chosen, next_real, result_real)
        result_imag = jnp.where(chosen, next_imag, result_imag)
        square_real, square_imag = rotate(square_real, square_imag, square_real, square_imag)
    return (result_real, result_imag)


def local(
    tokens,
    norm_gain,
    conv_value,
    conv_gate,
    state_feed,
    conv_taps,
    chan_gain,
    chan_shift,
    conv_project,
    decay_rate,
    frequency,
    input_real,
    input_imag,
    output_real,
    output_imag,
    skip_gain,
    state_value,
    state_gate,
    initial_state,
):
    highest = lax.Precision.HIGHEST
    floats = tokens.astype(jnp.float32)
    normed = (
        floats * lax.rsqrt(jnp.mean(floats * floats, axis=1, keepdims=True) + 1e-06) * norm_gain
    ).astype(jnp.bfloat16)
    length = tokens.shape[0]
    width = conv_value.shape[1]
    in_block = jnp.concatenate([conv_value, conv_gate, state_feed], axis=1)
    projected = jnp.dot(
        normed,
        lax.all_gather(in_block, "sp", axis=0, tiled=True),
        preferred_element_type=jnp.float32,
    )
    gated_linear = (projected[:, :width] * jax.nn.sigmoid(projected[:, width : 2 * width])).astype(
        jnp.bfloat16
    )
    state_drive = projected[:, 2 * width :].astype(jnp.bfloat16)
    kernel = conv_taps.shape[0]
    before = passed_along(gated_linear[length - (kernel - 1) :], "sp", 1)
    padded = jnp.concatenate([before, gated_linear], axis=0).astype(jnp.float32)
    conv_sum = jnp.zeros((length, width), jnp.float32)
    for offset in range(kernel):
        conv_sum = conv_sum + conv_taps[offset] * padded[offset : offset + length]
    conv_out = conv_sum.astype(jnp.bfloat16)
    seq_devices = lax.axis_size("sp")
    total_tokens = length * seq_devices
    groups, state_size, group_size = input_real.shape
    flat = groups * state_size
    rate_real = -decay_rate / total_tokens
    magnitude = jnp.exp(rate_real)
    step_real = magnitude * jnp.cos(frequency)
    step_imag = magnitude * jnp.sin(frequency)
    modulus = rate_real * rate_real + frequency * frequency
    lift_real = step_real - 1.0
    factor_real = (lift_real * rate_real + step_imag * frequency) / modulus
    factor_imag = (step_imag * rate_real - lift_real * frequency) / modulus
    drive_real = factor_real[..., None] * input_real - factor_imag[..., None] * input_imag
    drive_imag = factor_real[..., None] * input_imag + factor_imag[..., None] * input_real
    grouped = state_drive.astype(jnp.float32).reshape(length, groups, group_size)
    pushed_real = jnp.einsum("gph,tgh->tgp", drive_real, grouped, precision=highest).reshape(
        length, flat
    )
    pushed_imag = jnp.einsum("gph,tgh->tgp", drive_imag, grouped, precision=highest).reshape(
        length, flat
    )
    base_real = step_real.reshape(flat)
    base_imag = step_imag.reshape(flat)
    square_size = base_real * base_real + base_imag * base_imag
    back_real = base_real / square_size
    back_imag = -base_imag / square_size
    positions = lax.iota(jnp.int32, length)
    counted = positions + 1
    power_real, power_imag = power_table(base_real, base_imag, counted, length)
    undo_real, undo_imag = power_table(back_real, back_imag, counted, length)
    scaled_real, scaled_imag = rotate(undo_real, undo_imag, pushed_real, pushed_imag)
    lower = (positions[:, None] >= positions[None, :]).astype(jnp.float32)
    summed_real = jnp.dot(lower, scaled_real, precision=highest)
    summed_imag = jnp.dot(lower, scaled_imag, precision=highest)
    local_real, local_imag = rotate(power_real, power_imag, summed_real, summed_imag)
    span_real, span_imag = (power_real[-1], power_imag[-1])
    last_real, last_imag = (local_real[-1], local_imag[-1])
    start_real = initial_state[0].reshape(flat)
    start_imag = initial_state[1].reshape(flat)
    finals = lax.all_gather(jnp.stack([last_real, last_imag])[None], "sp", axis=0, tiled=True)
    position = lax.axis_index("sp")
    device_ids = lax.iota(jnp.int32, seq_devices)
    lag = jnp.maximum(position - 1 - device_ids, 0)
    weight_real, weight_imag = power_table(span_real, span_imag, lag, seq_devices)
    before_mask = (device_ids < position).astype(jnp.float32)[:, None]
    moved_real, moved_imag = rotate(weight_real, weight_imag, finals[:, 0], finals[:, 1])
    lead_real, lead_imag = power_table(
        span_real, span_imag, jnp.stack([position, jnp.int32(seq_devices)]), seq_devices
    )
    opening_real, opening_imag = rotate(lead_real[0], lead_imag[0], start_real, start_imag)
    entry_real = opening_real + jnp.sum(moved_real * before_mask, axis=0)
    entry_imag = opening_imag + jnp.sum(moved_imag * before_mask, axis=0)
    tail_real, tail_imag = power_table(
        span_real, span_imag, seq_devices - 1 - device_ids, seq_devices
    )
    carried_real, carried_imag = rotate(tail_real, tail_imag, finals[:, 0], finals[:, 1])
    closing_real, closing_imag = rotate(lead_real[1], lead_imag[1], start_real, start_imag)
    final_real = closing_real + jnp.sum(carried_real, axis=0)
    final_imag = closing_imag + jnp.sum(carried_imag, axis=0)
    final_state = jnp.stack([final_real, final_imag]).reshape(2, groups, state_size)
    state_real = (power_real * entry_real - power_imag * entry_imag + local_real).reshape(
        length, groups, state_size
    )
    state_imag = (power_real * entry_imag + power_imag * entry_real + local_imag).reshape(
        length, groups, state_size
    )
    response = jnp.einsum("ghp,tgp->tgh", output_real, state_real, precision=highest) - jnp.einsum(
        "ghp,tgp->tgh", output_imag, state_imag, precision=highest
    )
    response = response.reshape(length, groups * group_size) + skip_gain * state_drive.astype(
        jnp.float32
    )
    activated = jax.nn.gelu(response).astype(jnp.bfloat16)
    conv_rows, activated_rows = (
        lax.all_gather(conv_out, "tp", axis=1, tiled=True),
        lax.all_gather(activated, "tp", axis=1, tiled=True),
    )
    conv_full = conv_rows.astype(jnp.float32)
    row_mean = jnp.mean(conv_full, axis=1, keepdims=True)
    centred = conv_full - row_mean
    variance = jnp.mean(centred * centred, axis=1, keepdims=True)
    conv_act = jax.nn.silu(centred * lax.rsqrt(variance + 1e-05) * chan_gain + chan_shift).astype(
        jnp.bfloat16
    )
    columns = conv_project.shape[1]
    out_block = jnp.concatenate([conv_project, state_value, state_gate], axis=1)
    piece = lax.all_gather(out_block, "sp", axis=0, tiled=True)
    conv_branch = jnp.dot(conv_act, piece[:, :columns], preferred_element_type=jnp.float32)
    state_both = jnp.dot(activated_rows, piece[:, columns:], preferred_element_type=jnp.float32)
    mixer_out = (
        conv_branch + state_both[:, :columns] * jax.nn.sigmoid(state_both[:, columns:])
    ).astype(jnp.bfloat16)
    return (mixer_out, final_state)


def power_stack(base_real, base_imag, count):
    real, imag = (base_real[None], base_imag[None])
    while real.shape[0] < count:
        next_real, next_imag = rotate(real, imag, real[-1:], imag[-1:])
        real = jnp.concatenate([real, next_real], axis=0)
        imag = jnp.concatenate([imag, next_imag], axis=0)
    return (real[:count], imag[:count])


def block_diagonal(blocks):
    groups = blocks.shape[1]
    return blocks[:, :, :, None, :] * jnp.eye(groups, dtype=blocks.dtype)[None, :, None, :, None]


def chunk_matrices(decay_rate, frequency, input_real, input_imag, output_real, output_imag, total, chunk):
    highest = lax.Precision.HIGHEST
    groups, states, width = input_real.shape
    rate_real = -decay_rate / total
    magnitude = jnp.exp(rate_real)
    step_real = magnitude * jnp.cos(frequency)
    step_imag = magnitude * jnp.sin(frequency)
    modulus = rate_real * rate_real + frequency * frequency
    lift_real = step_real - 1.0
    factor_real = (lift_real * rate_real + step_imag * frequency) / modulus
    factor_imag = (step_imag * rate_real - lift_real * frequency) / modulus
    drive_real = factor_real[..., None] * input_real - factor_imag[..., None] * input_imag
    drive_imag = factor_real[..., None] * input_imag + factor_imag[..., None] * input_real
    power_real, power_imag = power_stack(step_real, step_imag, chunk)
    whole_real = jnp.concatenate([jnp.ones_like(step_real)[None], power_real], axis=0)
    whole_imag = jnp.concatenate([jnp.zeros_like(step_imag)[None], power_imag], axis=0)
    back_real = whole_real[:chunk][::-1, :, :, None]
    back_imag = whole_imag[:chunk][::-1, :, :, None]
    push_real, push_imag = rotate(back_real, back_imag, drive_real[None], drive_imag[None])
    push = [
        block_diagonal(value.transpose(0, 1, 3, 2)).reshape(chunk * groups * width, groups * states)
        for value in (push_real, push_imag)
    ]
    push = jnp.concatenate(push, axis=1)
    out_real, out_imag = rotate(
        output_real[None], output_imag[None], whole_real[:, :, None, :], whole_imag[:, :, None, :]
    )
    emit = [
        block_diagonal(value.transpose(1, 3, 0, 2).reshape(1, groups, states, chunk * width))
        for value in (out_real[1:], -out_imag[1:])
    ]
    emit = [
        value.reshape(groups, states, groups, chunk, width)
        .transpose(0, 1, 3, 2, 4)
        .reshape(groups * states, chunk * groups * width)
        for value in emit
    ]
    emit = jnp.concatenate(emit, axis=0)
    response = jnp.einsum(
        "dghp,gpi->dgih", out_real[:chunk], drive_real, precision=highest
    ) - jnp.einsum("dghp,gpi->dgih", out_imag[:chunk], drive_imag, precision=highest)
    spread = block_diagonal(response).reshape(chunk, groups * width, groups * width)
    spread = spread.transpose(1, 0, 2).reshape(groups * width, chunk * groups * width)
    padded = jnp.concatenate([jnp.zeros_like(spread), spread], axis=1)
    span = groups * width
    full = chunk * span
    inside = jnp.concatenate(
        [padded[:, full - place * span : 2 * full - place * span] for place in range(chunk)], axis=0
    )
    return (power_real[-1].reshape(-1), power_imag[-1].reshape(-1), push, emit, inside)


def recurrence(feed, skip_gain, start, matrices, chunk):
    highest = lax.Precision.HIGHEST
    span_real, span_imag, push, emit, inside = matrices
    length, width = feed.shape
    count = length // chunk
    rows = feed.reshape(count, chunk * width).astype(jnp.float32)
    pushed = jnp.dot(rows, push, precision=highest)
    flat = span_real.shape[0]
    first_real, first_imag = rotate(span_real, span_imag, start[0], start[1])
    head = jnp.concatenate([first_real, first_imag])[None]
    pushed = jnp.concatenate([pushed[:1] + head, pushed[1:]], axis=0)
    real, imag = (pushed[:, :flat], pushed[:, flat:])
    shift = 1
    while shift < count:
        moved_real = jnp.pad(real[:-shift], ((shift, 0), (0, 0)))
        moved_imag = jnp.pad(imag[:-shift], ((shift, 0), (0, 0)))
        add_real, add_imag = rotate(span_real, span_imag, moved_real, moved_imag)
        real, imag = (real + add_real, imag + add_imag)
        span_real, span_imag = rotate(span_real, span_imag, span_real, span_imag)
        shift *= 2
    entry_real = jnp.concatenate([start[0][None], real[:-1]], axis=0)
    entry_imag = jnp.concatenate([start[1][None], imag[:-1]], axis=0)
    entry = jnp.concatenate([entry_real, entry_imag], axis=1)
    response = jnp.dot(rows, inside, precision=highest) + jnp.dot(entry, emit, precision=highest)
    response = response + jnp.tile(skip_gain, chunk) * rows
    activated = jax.nn.gelu(response).astype(jnp.bfloat16).reshape(length, width)
    return (activated, jnp.stack([real[-1], imag[-1]]))


def remote(source, target, send_sem, recv_sem, device):
    return pltpu.make_async_remote_copy(
        src_ref=source,
        dst_ref=target,
        send_sem=send_sem,
        recv_sem=recv_sem,
        device_id=device,
        device_id_type=pl.DeviceIdType.MESH,
    )


def plane_neighbours(inner, core):
    flip_x = inner + 1 - 2 * (inner % 2)
    flip_y = inner + 2 - 4 * (inner // 2)
    first = flip_x * (1 - core) + flip_y * core
    second = flip_y * (1 - core) + flip_x * core
    return (first, second, 3 - inner)


def entry_kernel(
    depth, own_ref, in_ref, out_ref, all_ref, taken_ref, moved_ref, sent, landed, in_sent, in_landed,
    out_sent, out_landed, local_sem
):
    outer, inner, core = (lax.axis_index("outer"), lax.axis_index("inner"), lax.axis_index("tp"))
    first, second, opposite = plane_neighbours(inner, core)
    length = own_ref.shape[0]
    devices = 4 * depth
    here = outer * 4 + inner
    half = devices // 2
    target_core = here // half

    def slot(index):
        return all_ref.at[pl.ds(pl.multiple_of(index * length, length), length)]

    def send(index, lane, device, source=None):
        return remote(
            slot(index) if source is None else source,
            slot(index),
            sent.at[index, lane],
            landed.at[index],
            device,
        )

    def arrived(index):
        send(index, 0, (outer, first, core)).wait_recv()

    def spread(index, source=None):
        send(index, 0, (outer, first, core), source).start()
        send(index, 1, (outer, second, core), source).start()

    up, down = ((outer + 1, inner, core), (outer - 1, inner, core))

    @pl.when(outer < depth - 1)
    def _():
        send(here, 2, up, own_ref).start()

    @pl.when(outer > 0)
    def _():
        send(here, 3, down, own_ref).start()

    spread(here, own_ref)
    keep = pltpu.make_async_copy(own_ref, slot(here), local_sem.at[0])
    keep.start()
    place = core * half + here % half

    def in_copy(offset):
        other = (here + offset) % devices
        return remote(
            in_ref.at[other],
            taken_ref.at[place],
            in_sent.at[offset],
            in_landed.at[place],
            (other // 4, other % 4, target_core),
        )

    in_keep = pltpu.make_async_copy(in_ref.at[here], taken_ref.at[place], local_sem.at[1])

    @pl.when(core == target_core)
    def _():
        in_keep.start()

    @pl.when(core != target_core)
    def _():
        in_copy(0).start()

    for offset in range(1, devices):
        in_copy(offset).start()

    out_keep = pltpu.make_async_copy(out_ref.at[inner], moved_ref.at[inner], local_sem.at[2])
    out_keep.start()

    def out_copy(offset):
        other = (inner + offset) % 4
        return remote(
            out_ref.at[other],
            moved_ref.at[inner],
            out_sent.at[offset - 1],
            out_landed.at[inner],
            (outer, other, core),
        )

    for offset in range(1, 4):
        out_copy(offset).start()

    def side(z):
        index = z * 4 + first
        arrived(index)
        send(index, 1, (outer, second, core)).start()

    side(outer)
    for step in range(1, depth):
        below, above = (outer - step, outer + step)

        @pl.when(below >= 0)
        def _():
            index = below * 4 + inner
            arrived(index)

            @pl.when(outer < depth - 1)
            def _():
                send(index, 2, up).start()

            spread(index)

        @pl.when(above < depth)
        def _():
            index = above * 4 + inner
            arrived(index)

            @pl.when(outer > 0)
            def _():
                send(index, 3, down).start()

            spread(index)

        @pl.when(below >= 0)
        def _():
            side(below)

        @pl.when(above < depth)
        def _():
            side(above)

    for z in range(depth):
        arrived(z * 4 + second)
        arrived(z * 4 + opposite)

    for z in range(depth):
        index = z * 4 + inner
        send(index, 0, (outer, first, core)).wait_send()
        send(index, 1, (outer, second, core)).wait_send()
        send(z * 4 + first, 1, (outer, second, core)).wait_send()

        @pl.when(jnp.logical_and(outer < depth - 1, z <= outer))
        def _():
            send(index, 2, up).wait_send()

        @pl.when(jnp.logical_and(outer > 0, z >= outer))
        def _():
            send(index, 3, down).wait_send()

    keep.wait()

    @pl.when(core == target_core)
    def _():
        in_keep.wait()

    @pl.when(core != target_core)
    def _():
        in_copy(0).wait_send()

    for offset in range(1, devices):
        in_copy(offset).wait_send()

    def in_wait(index):
        remote(
            in_ref.at[0],
            taken_ref.at[index],
            in_sent.at[0],
            in_landed.at[index],
            (outer, first, core),
        ).wait_recv()

    for lane in range(2):
        for index in range(half):
            local_one = jnp.logical_and(here == core * half + index, core == lane)

            @pl.when(jnp.logical_not(local_one))
            def _():
                in_wait(lane * half + index)

    out_keep.wait()
    for offset in range(1, 4):
        out_copy(offset).wait_send()
    for offset in range(1, 4):
        other = (inner + offset) % 4
        remote(
            out_ref.at[0],
            moved_ref.at[other],
            out_sent.at[0],
            out_landed.at[other],
            (outer, first, core),
        ).wait_recv()


def entry_exchange(own_half, in_block, out_block, depth):
    devices = 4 * depth
    length, half = own_half.shape
    any_spec = pl.BlockSpec(memory_space=pl.ANY)
    dma = pltpu.SemaphoreType.DMA
    return pl.pallas_call(
        functools.partial(entry_kernel, depth),
        out_shape=(
            jax.ShapeDtypeStruct((devices * length, half), own_half.dtype),
            jax.ShapeDtypeStruct(in_block.shape, in_block.dtype),
            jax.ShapeDtypeStruct(out_block.shape, out_block.dtype),
        ),
        in_specs=[any_spec] * 3,
        out_specs=(any_spec,) * 3,
        scratch_shapes=[
            dma((devices, 4)),
            dma((devices,)),
            dma((devices,)),
            dma((devices,)),
            dma((3,)),
            dma((4,)),
            dma((3,)),
        ],
        compiler_params=pltpu.CompilerParams(has_side_effects=True),
        cost_estimate=pl.CostEstimate(flops=0, bytes_accessed=0, transcendentals=0),
    )(own_half, in_block, out_block)


def middle_kernel(depth, mixed_ref, last_ref, turned_ref, states_ref, sent, landed, last_sent, last_landed, local_sem):
    outer, inner, core = (lax.axis_index("outer"), lax.axis_index("inner"), lax.axis_index("tp"))
    devices = 4 * depth
    here = outer * 4 + inner
    keep = pltpu.make_async_copy(mixed_ref.at[here], turned_ref.at[here], local_sem.at[0])
    keep_last = pltpu.make_async_copy(last_ref, states_ref.at[here], local_sem.at[1])
    keep.start()
    keep_last.start()

    def copies(offset):
        other = (here + offset) % devices
        device = (other // 4, other % 4, core)
        return (
            remote(
                mixed_ref.at[other], turned_ref.at[here], sent.at[offset], landed.at[here], device
            ),
            remote(
                last_ref, states_ref.at[here], last_sent.at[offset], last_landed.at[here], device
            ),
        )

    for offset in range(1, devices):
        for copy in copies(offset):
            copy.start()
    keep.wait()
    keep_last.wait()
    for offset in range(1, devices):
        for copy in copies(offset):
            copy.wait_send()
    for offset in range(1, devices):
        other = (here + offset) % devices
        device = (other // 4, other % 4, core)
        remote(
            mixed_ref.at[other], turned_ref.at[other], sent.at[offset], landed.at[other], device
        ).wait_recv()
        remote(
            last_ref, states_ref.at[other], last_sent.at[offset], last_landed.at[other], device
        ).wait_recv()


def middle_exchange(mixed, last, depth):
    devices = 4 * depth
    any_spec = pl.BlockSpec(memory_space=pl.ANY)
    dma = pltpu.SemaphoreType.DMA
    return pl.pallas_call(
        functools.partial(middle_kernel, depth),
        out_shape=(
            jax.ShapeDtypeStruct(mixed.shape, mixed.dtype),
            jax.ShapeDtypeStruct((devices,) + last.shape, last.dtype),
        ),
        in_specs=[any_spec] * 2,
        out_specs=(any_spec,) * 2,
        scratch_shapes=[dma((devices,))] * 4 + [dma((2,))],
        compiler_params=pltpu.CompilerParams(has_side_effects=True),
    )(mixed, last)


def channel_local(
    tokens,
    norm_gain,
    conv_value,
    conv_gate,
    state_feed,
    conv_taps,
    chan_gain,
    chan_shift,
    conv_project,
    decay_rate,
    frequency,
    input_real,
    input_imag,
    output_real,
    output_imag,
    skip_gain,
    state_value,
    state_gate,
    initial_state,
):
    seq = ("outer", "inner")
    devices = lax.axis_size("outer") * lax.axis_size("inner")
    inner = lax.axis_size("inner")
    position = lax.axis_index("outer") * inner + lax.axis_index("inner")
    core = lax.axis_index("tp")
    swap = [(0, 1), (1, 0)]
    local_length, model = tokens.shape
    total = local_length * devices
    half = model // 2
    floats = tokens.astype(jnp.float32)
    normed = (
        floats * lax.rsqrt(jnp.mean(floats * floats, axis=1, keepdims=True) + 1e-06) * norm_gain
    ).astype(jnp.bfloat16)
    own_half = lax.dynamic_slice_in_dim(normed, core * half, half, axis=1)
    rows, wide = conv_value.shape
    share = wide // devices
    in_block = jnp.stack([conv_value, conv_gate, state_feed], axis=1)
    in_block = in_block.reshape(rows, 3, devices, share).transpose(2, 0, 1, 3)
    in_block = in_block.reshape(devices, rows, 3 * share)
    out_rows, columns = conv_project.shape
    piece = columns // inner
    out_block = jnp.stack([conv_project, state_value, state_gate], axis=1)
    out_block = out_block.reshape(out_rows, 3, inner, piece).transpose(2, 0, 1, 3)
    out_block = out_block.reshape(inner, out_rows, 3 * piece)
    all_half, in_block, out_block = entry_exchange(
        own_half, in_block, out_block, lax.axis_size("outer")
    )
    in_block = in_block.reshape(2, half, 3 * share)
    kept = lax.dynamic_index_in_dim(in_block, core, axis=0, keepdims=False)
    taken = lax.dynamic_index_in_dim(in_block, 1 - core, axis=0, keepdims=False)
    out_block = lax.all_gather(
        out_block.reshape(inner * out_rows, 3 * piece), "outer", axis=0, tiled=True
    )
    groups = decay_rate.shape[0] // devices
    chunk = 16

    def own(value, axis=0, size=groups):
        return lax.dynamic_slice_in_dim(value, position * size, size, axis=axis)

    matrices = chunk_matrices(
        own(decay_rate),
        own(frequency),
        own(input_real),
        own(input_imag),
        own(output_real),
        own(output_imag),
        total,
        chunk,
    )
    other = lax.ppermute(jnp.dot(all_half, taken, preferred_element_type=jnp.float32), "tp", swap)
    projected = jnp.dot(all_half, kept, preferred_element_type=jnp.float32) + other
    gated = (projected[:, :share] * jax.nn.sigmoid(projected[:, share : 2 * share])).astype(
        jnp.bfloat16
    )
    feed = projected[:, 2 * share :].astype(jnp.bfloat16)
    kernel = conv_taps.shape[0]
    taps = own(conv_taps, 1, share)
    padded = jnp.pad(gated, ((kernel - 1, 0), (0, 0))).astype(jnp.float32)
    conv_sum = jnp.zeros((total, share), jnp.float32)
    for offset in range(kernel):
        conv_sum = conv_sum + taps[offset] * padded[offset : offset + total]
    conv_out = conv_sum.astype(jnp.bfloat16)
    start = own(initial_state, 1).reshape(2, -1)
    activated, last = recurrence(feed, own(skip_gain, 0, share), start, matrices, chunk)
    states = initial_state.shape[2]
    mixed = jnp.concatenate([conv_out, activated], axis=1).reshape(devices, local_length, 2 * share)
    mixed, last = middle_exchange(mixed, last.reshape(-1, 128), lax.axis_size("outer"))
    mixed = mixed.transpose(1, 0, 2)
    final_state = last.reshape(devices, 2, groups, states).transpose(1, 0, 2, 3)
    final_state = final_state.reshape(initial_state.shape)
    conv_full = mixed[:, :, :share].reshape(local_length, wide).astype(jnp.float32)
    active = mixed[:, :, share:].reshape(local_length, wide)
    own_mean = jnp.mean(conv_full, axis=1, keepdims=True)
    deviation = conv_full - own_mean
    own_spread = jnp.mean(deviation * deviation, axis=1, keepdims=True)
    peer = lax.ppermute(jnp.concatenate([own_mean, own_spread], axis=1), "tp", swap)
    row_mean = 0.5 * (own_mean + peer[:, :1])
    gap = 0.5 * (own_mean - peer[:, :1])
    variance = 0.5 * (own_spread + peer[:, 1:]) + gap * gap
    gain = lax.dynamic_slice_in_dim(chan_gain, core * wide, wide, axis=0)
    bias = lax.dynamic_slice_in_dim(chan_shift, core * wide, wide, axis=0)
    conv_act = jax.nn.silu(
        (conv_full - row_mean) * lax.rsqrt(variance + 1e-05) * gain + bias
    ).astype(jnp.bfloat16)
    both = jnp.stack([conv_act, active], axis=0)
    both = lax.all_gather(both, "inner", axis=1, tiled=True)
    both = lax.all_gather(both, "tp", axis=2, tiled=True)
    conv_branch = jnp.dot(both[0], out_block[:, :piece], preferred_element_type=jnp.float32)
    state_both = jnp.dot(both[1], out_block[:, piece:], preferred_element_type=jnp.float32)
    mixer = (conv_branch + state_both[:, :piece] * jax.nn.sigmoid(state_both[:, piece:])).astype(
        jnp.bfloat16
    )
    mixer = mixer.reshape(inner, local_length, piece)
    mixer = lax.all_to_all(mixer, "inner", 0, 0, tiled=True)
    mixer_out = mixer.transpose(1, 0, 2).reshape(local_length, columns)
    return (mixer_out, final_state)


def specs_of(seq):
    in_specs = (
        P(seq, None),
        P(),
        P(seq, "tp"),
        P(seq, "tp"),
        P(seq, "tp"),
        P(None, "tp"),
        P(),
        P(),
        P(seq, "tp"),
        P("tp", None),
        P("tp", None),
        P("tp", None, None),
        P("tp", None, None),
        P("tp", None, None),
        P("tp", None, None),
        P("tp"),
        P(seq, "tp"),
        P(seq, "tp"),
        P(None, "tp", None),
    )
    return (in_specs, (P(seq, "tp"), P(None, "tp", None)))


def solution(mesh):
    seq_devices, cores = (mesh.shape["sp"], mesh.shape["tp"])
    fine = jax.sharding.Mesh(
        mesh.devices.reshape(seq_devices // 4, 4, cores), ("outer", "inner", "tp")
    )

    def run(*args):
        groups = args[9].shape[0]
        if cores == 2 and groups % (cores * seq_devices) == 0:
            in_specs, out_specs = specs_of(("outer", "inner"))
            body = jax.shard_map(
                channel_local, mesh=fine, in_specs=in_specs, out_specs=out_specs, check_vma=False
            )
        else:
            in_specs, out_specs = specs_of("sp")
            body = jax.shard_map(
                local, mesh=mesh, in_specs=in_specs, out_specs=out_specs, check_vma=False
            )
        return body(*args)

    return run
```

```python
import functools
import jax
import jax.numpy as jnp
from jax import lax
from jax.experimental import pallas as pl
from jax.experimental.pallas import tpu as pltpu
from jax.sharding import PartitionSpec as P


def passed_along(value, axis, steps):
    count = lax.axis_size(axis)
    leading, last = (max(0, -steps), min(count, count - steps))
    return lax.ppermute(value, axis, [(source, source + steps) for source in range(leading, last)])


def rotate(first_real, first_imag, second_real, second_imag):
    return (
        first_real * second_real - first_imag * second_imag,
        first_real * second_imag + first_imag * second_real,
    )


def power_table(base_real, base_imag, exponent, largest):
    result_real = jnp.ones((exponent.shape[0], base_real.shape[0]), jnp.float32)
    result_imag = jnp.zeros((exponent.shape[0], base_real.shape[0]), jnp.float32)
    square_real, square_imag = (base_real, base_imag)
    for place in range(max(largest, 1).bit_length()):
        chosen = (exponent >> place & 1 == 1)[:, None]
        next_real, next_imag = rotate(result_real, result_imag, square_real, square_imag)
        result_real = jnp.where(chosen, next_real, result_real)
        result_imag = jnp.where(chosen, next_imag, result_imag)
        square_real, square_imag = rotate(square_real, square_imag, square_real, square_imag)
    return (result_real, result_imag)


def local(
    tokens,
    norm_gain,
    conv_value,
    conv_gate,
    state_feed,
    conv_taps,
    chan_gain,
    chan_shift,
    conv_project,
    decay_rate,
    frequency,
    input_real,
    input_imag,
    output_real,
    output_imag,
    skip_gain,
    state_value,
    state_gate,
    initial_state,
):
    highest = lax.Precision.HIGHEST
    floats = tokens.astype(jnp.float32)
    normed = (
        floats * lax.rsqrt(jnp.mean(floats * floats, axis=1, keepdims=True) + 1e-06) * norm_gain
    ).astype(jnp.bfloat16)
    length = tokens.shape[0]
    width = conv_value.shape[1]
    in_block = jnp.concatenate([conv_value, conv_gate, state_feed], axis=1)
    projected = jnp.dot(
        normed,
        lax.all_gather(in_block, "sp", axis=0, tiled=True),
        preferred_element_type=jnp.float32,
    )
    gated_linear = (projected[:, :width] * jax.nn.sigmoid(projected[:, width : 2 * width])).astype(
        jnp.bfloat16
    )
    state_drive = projected[:, 2 * width :].astype(jnp.bfloat16)
    kernel = conv_taps.shape[0]
    before = passed_along(gated_linear[length - (kernel - 1) :], "sp", 1)
    padded = jnp.concatenate([before, gated_linear], axis=0).astype(jnp.float32)
    conv_sum = jnp.zeros((length, width), jnp.float32)
    for offset in range(kernel):
        conv_sum = conv_sum + conv_taps[offset] * padded[offset : offset + length]
    conv_out = conv_sum.astype(jnp.bfloat16)
    seq_devices = lax.axis_size("sp")
    total_tokens = length * seq_devices
    groups, state_size, group_size = input_real.shape
    flat = groups * state_size
    rate_real = -decay_rate / total_tokens
    magnitude = jnp.exp(rate_real)
    step_real = magnitude * jnp.cos(frequency)
    step_imag = magnitude * jnp.sin(frequency)
    modulus = rate_real * rate_real + frequency * frequency
    lift_real = step_real - 1.0
    factor_real = (lift_real * rate_real + step_imag * frequency) / modulus
    factor_imag = (step_imag * rate_real - lift_real * frequency) / modulus
    drive_real = factor_real[..., None] * input_real - factor_imag[..., None] * input_imag
    drive_imag = factor_real[..., None] * input_imag + factor_imag[..., None] * input_real
    grouped = state_drive.astype(jnp.float32).reshape(length, groups, group_size)
    pushed_real = jnp.einsum("gph,tgh->tgp", drive_real, grouped, precision=highest).reshape(
        length, flat
    )
    pushed_imag = jnp.einsum("gph,tgh->tgp", drive_imag, grouped, precision=highest).reshape(
        length, flat
    )
    base_real = step_real.reshape(flat)
    base_imag = step_imag.reshape(flat)
    square_size = base_real * base_real + base_imag * base_imag
    back_real = base_real / square_size
    back_imag = -base_imag / square_size
    positions = lax.iota(jnp.int32, length)
    counted = positions + 1
    power_real, power_imag = power_table(base_real, base_imag, counted, length)
    undo_real, undo_imag = power_table(back_real, back_imag, counted, length)
    scaled_real, scaled_imag = rotate(undo_real, undo_imag, pushed_real, pushed_imag)
    lower = (positions[:, None] >= positions[None, :]).astype(jnp.float32)
    summed_real = jnp.dot(lower, scaled_real, precision=highest)
    summed_imag = jnp.dot(lower, scaled_imag, precision=highest)
    local_real, local_imag = rotate(power_real, power_imag, summed_real, summed_imag)
    span_real, span_imag = (power_real[-1], power_imag[-1])
    last_real, last_imag = (local_real[-1], local_imag[-1])
    start_real = initial_state[0].reshape(flat)
    start_imag = initial_state[1].reshape(flat)
    finals = lax.all_gather(jnp.stack([last_real, last_imag])[None], "sp", axis=0, tiled=True)
    position = lax.axis_index("sp")
    device_ids = lax.iota(jnp.int32, seq_devices)
    lag = jnp.maximum(position - 1 - device_ids, 0)
    weight_real, weight_imag = power_table(span_real, span_imag, lag, seq_devices)
    before_mask = (device_ids < position).astype(jnp.float32)[:, None]
    moved_real, moved_imag = rotate(weight_real, weight_imag, finals[:, 0], finals[:, 1])
    lead_real, lead_imag = power_table(
        span_real, span_imag, jnp.stack([position, jnp.int32(seq_devices)]), seq_devices
    )
    opening_real, opening_imag = rotate(lead_real[0], lead_imag[0], start_real, start_imag)
    entry_real = opening_real + jnp.sum(moved_real * before_mask, axis=0)
    entry_imag = opening_imag + jnp.sum(moved_imag * before_mask, axis=0)
    tail_real, tail_imag = power_table(
        span_real, span_imag, seq_devices - 1 - device_ids, seq_devices
    )
    carried_real, carried_imag = rotate(tail_real, tail_imag, finals[:, 0], finals[:, 1])
    closing_real, closing_imag = rotate(lead_real[1], lead_imag[1], start_real, start_imag)
    final_real = closing_real + jnp.sum(carried_real, axis=0)
    final_imag = closing_imag + jnp.sum(carried_imag, axis=0)
    final_state = jnp.stack([final_real, final_imag]).reshape(2, groups, state_size)
    state_real = (power_real * entry_real - power_imag * entry_imag + local_real).reshape(
        length, groups, state_size
    )
    state_imag = (power_real * entry_imag + power_imag * entry_real + local_imag).reshape(
        length, groups, state_size
    )
    response = jnp.einsum("ghp,tgp->tgh", output_real, state_real, precision=highest) - jnp.einsum(
        "ghp,tgp->tgh", output_imag, state_imag, precision=highest
    )
    response = response.reshape(length, groups * group_size) + skip_gain * state_drive.astype(
        jnp.float32
    )
    activated = jax.nn.gelu(response).astype(jnp.bfloat16)
    conv_rows, activated_rows = (
        lax.all_gather(conv_out, "tp", axis=1, tiled=True),
        lax.all_gather(activated, "tp", axis=1, tiled=True),
    )
    conv_full = conv_rows.astype(jnp.float32)
    row_mean = jnp.mean(conv_full, axis=1, keepdims=True)
    centred = conv_full - row_mean
    variance = jnp.mean(centred * centred, axis=1, keepdims=True)
    conv_act = jax.nn.silu(centred * lax.rsqrt(variance + 1e-05) * chan_gain + chan_shift).astype(
        jnp.bfloat16
    )
    columns = conv_project.shape[1]
    out_block = jnp.concatenate([conv_project, state_value, state_gate], axis=1)
    piece = lax.all_gather(out_block, "sp", axis=0, tiled=True)
    conv_branch = jnp.dot(conv_act, piece[:, :columns], preferred_element_type=jnp.float32)
    state_both = jnp.dot(activated_rows, piece[:, columns:], preferred_element_type=jnp.float32)
    mixer_out = (
        conv_branch + state_both[:, :columns] * jax.nn.sigmoid(state_both[:, columns:])
    ).astype(jnp.bfloat16)
    return (mixer_out, final_state)


def power_stack(base_real, base_imag, count):
    real, imag = (base_real[None], base_imag[None])
    while real.shape[0] < count:
        next_real, next_imag = rotate(real, imag, real[-1:], imag[-1:])
        real = jnp.concatenate([real, next_real], axis=0)
        imag = jnp.concatenate([imag, next_imag], axis=0)
    return (real[:count], imag[:count])


def block_diagonal(blocks):
    groups = blocks.shape[1]
    return blocks[:, :, :, None, :] * jnp.eye(groups, dtype=blocks.dtype)[None, :, None, :, None]


def chunk_matrices(decay_rate, frequency, input_real, input_imag, output_real, output_imag, total, chunk):
    highest = lax.Precision.HIGHEST
    groups, states, width = input_real.shape
    rate_real = -decay_rate / total
    magnitude = jnp.exp(rate_real)
    step_real = magnitude * jnp.cos(frequency)
    step_imag = magnitude * jnp.sin(frequency)
    modulus = rate_real * rate_real + frequency * frequency
    lift_real = step_real - 1.0
    factor_real = (lift_real * rate_real + step_imag * frequency) / modulus
    factor_imag = (step_imag * rate_real - lift_real * frequency) / modulus
    drive_real = factor_real[..., None] * input_real - factor_imag[..., None] * input_imag
    drive_imag = factor_real[..., None] * input_imag + factor_imag[..., None] * input_real
    power_real, power_imag = power_stack(step_real, step_imag, chunk)
    whole_real = jnp.concatenate([jnp.ones_like(step_real)[None], power_real], axis=0)
    whole_imag = jnp.concatenate([jnp.zeros_like(step_imag)[None], power_imag], axis=0)
    back_real = whole_real[:chunk][::-1, :, :, None]
    back_imag = whole_imag[:chunk][::-1, :, :, None]
    push_real, push_imag = rotate(back_real, back_imag, drive_real[None], drive_imag[None])
    push = [
        block_diagonal(value.transpose(0, 1, 3, 2)).reshape(chunk * groups * width, groups * states)
        for value in (push_real, push_imag)
    ]
    push = jnp.concatenate(push, axis=1)
    out_real, out_imag = rotate(
        output_real[None], output_imag[None], whole_real[:, :, None, :], whole_imag[:, :, None, :]
    )
    emit = [
        block_diagonal(value.transpose(1, 3, 0, 2).reshape(1, groups, states, chunk * width))
        for value in (out_real[1:], -out_imag[1:])
    ]
    emit = [
        value.reshape(groups, states, groups, chunk, width)
        .transpose(0, 1, 3, 2, 4)
        .reshape(groups * states, chunk * groups * width)
        for value in emit
    ]
    emit = jnp.concatenate(emit, axis=0)
    response = jnp.einsum(
        "dghp,gpi->dgih", out_real[:chunk], drive_real, precision=highest
    ) - jnp.einsum("dghp,gpi->dgih", out_imag[:chunk], drive_imag, precision=highest)
    spread = block_diagonal(response).reshape(chunk, groups * width, groups * width)
    spread = spread.transpose(1, 0, 2).reshape(groups * width, chunk * groups * width)
    padded = jnp.concatenate([jnp.zeros_like(spread), spread], axis=1)
    span = groups * width
    full = chunk * span
    inside = jnp.concatenate(
        [padded[:, full - place * span : 2 * full - place * span] for place in range(chunk)], axis=0
    )
    return (power_real[-1].reshape(-1), power_imag[-1].reshape(-1), push, emit, inside)


def recurrence(feed, skip_gain, start, matrices, chunk):
    highest = lax.Precision.HIGHEST
    span_real, span_imag, push, emit, inside = matrices
    length, width = feed.shape
    count = length // chunk
    rows = feed.reshape(count, chunk * width).astype(jnp.float32)
    pushed = jnp.dot(rows, push, precision=highest)
    flat = span_real.shape[0]
    first_real, first_imag = rotate(span_real, span_imag, start[0], start[1])
    head = jnp.concatenate([first_real, first_imag])[None]
    pushed = jnp.concatenate([pushed[:1] + head, pushed[1:]], axis=0)
    real, imag = (pushed[:, :flat], pushed[:, flat:])
    shift = 1
    while shift < count:
        moved_real = jnp.pad(real[:-shift], ((shift, 0), (0, 0)))
        moved_imag = jnp.pad(imag[:-shift], ((shift, 0), (0, 0)))
        add_real, add_imag = rotate(span_real, span_imag, moved_real, moved_imag)
        real, imag = (real + add_real, imag + add_imag)
        span_real, span_imag = rotate(span_real, span_imag, span_real, span_imag)
        shift *= 2
    entry_real = jnp.concatenate([start[0][None], real[:-1]], axis=0)
    entry_imag = jnp.concatenate([start[1][None], imag[:-1]], axis=0)
    entry = jnp.concatenate([entry_real, entry_imag], axis=1)
    response = jnp.dot(rows, inside, precision=highest) + jnp.dot(entry, emit, precision=highest)
    response = response + jnp.tile(skip_gain, chunk) * rows
    activated = jax.nn.gelu(response).astype(jnp.bfloat16).reshape(length, width)
    return (activated, jnp.stack([real[-1], imag[-1]]))


def remote(source, target, send_sem, recv_sem, device):
    return pltpu.make_async_remote_copy(
        src_ref=source,
        dst_ref=target,
        send_sem=send_sem,
        recv_sem=recv_sem,
        device_id=device,
        device_id_type=pl.DeviceIdType.MESH,
    )


def plane_neighbours(inner, core):
    flip_x = inner + 1 - 2 * (inner % 2)
    flip_y = inner + 2 - 4 * (inner // 2)
    first = flip_x * (1 - core) + flip_y * core
    second = flip_y * (1 - core) + flip_x * core
    return (first, second, 3 - inner)


def entry_kernel(
    depth, own_ref, in_ref, project_ref, value_ref, gate_ref, all_ref, taken_ref, moved_ref, sent,
    landed, in_sent, in_landed, out_sent, out_landed, local_sem
):
    outer, inner, core = (lax.axis_index("outer"), lax.axis_index("inner"), lax.axis_index("tp"))
    first, second, opposite = plane_neighbours(inner, core)
    length = own_ref.shape[0]
    devices = 4 * depth
    here = outer * 4 + inner
    half = devices // 2
    target_core = here // half

    def slot(index):
        return all_ref.at[pl.ds(pl.multiple_of(index * length, length), length)]

    def send(index, lane, device, source=None):
        return remote(
            slot(index) if source is None else source,
            slot(index),
            sent.at[index, lane],
            landed.at[index],
            device,
        )

    def arrived(index):
        send(index, 0, (outer, first, core)).wait_recv()

    def spread(index, source=None):
        send(index, 0, (outer, first, core), source).start()
        send(index, 1, (outer, second, core), source).start()

    up, down = ((outer + 1, inner, core), (outer - 1, inner, core))

    @pl.when(outer < depth - 1)
    def _():
        send(here, 2, up, own_ref).start()

    @pl.when(outer > 0)
    def _():
        send(here, 3, down, own_ref).start()

    spread(here, own_ref)
    keep = pltpu.make_async_copy(own_ref, slot(here), local_sem.at[0])
    keep.start()
    place = core * half + here % half

    def in_copy(offset):
        other = (here + offset) % devices
        return remote(
            in_ref.at[other],
            taken_ref.at[place],
            in_sent.at[offset],
            in_landed.at[place],
            (other // 4, other % 4, target_core),
        )

    in_keep = pltpu.make_async_copy(in_ref.at[here], taken_ref.at[place], local_sem.at[1])

    @pl.when(core == target_core)
    def _():
        in_keep.start()

    @pl.when(core != target_core)
    def _():
        in_copy(0).start()

    for offset in range(1, devices):
        in_copy(offset).start()

    out_refs = (project_ref, value_ref, gate_ref)
    out_rows, columns = project_ref.shape
    piece = columns // 4

    def out_from(which, other):
        return out_refs[which].at[:, pl.ds(pl.multiple_of(other * piece, piece), piece)]

    def out_to(which, origin):
        rows = pl.ds(pl.multiple_of(origin * out_rows, out_rows), out_rows)
        return moved_ref.at[rows, pl.ds(which * piece, piece)]

    def out_keep(which):
        return pltpu.make_async_copy(
            out_from(which, inner), out_to(which, inner), local_sem.at[2 + which]
        )

    def out_copy(which, offset):
        other = (inner + offset) % 4
        return remote(
            out_from(which, other),
            out_to(which, inner),
            out_sent.at[which, offset],
            out_landed.at[which, inner],
            (outer, other, core),
        )

    for which in range(3):
        out_keep(which).start()
        for offset in range(1, 4):
            out_copy(which, offset).start()

    def side(z):
        index = z * 4 + first
        arrived(index)
        send(index, 1, (outer, second, core)).start()

    side(outer)
    for step in range(1, depth):
        below, above = (outer - step, outer + step)

        @pl.when(below >= 0)
        def _():
            index = below * 4 + inner
            arrived(index)

            @pl.when(outer < depth - 1)
            def _():
                send(index, 2, up).start()

            spread(index)

        @pl.when(above < depth)
        def _():
            index = above * 4 + inner
            arrived(index)

            @pl.when(outer > 0)
            def _():
                send(index, 3, down).start()

            spread(index)

        @pl.when(below >= 0)
        def _():
            side(below)

        @pl.when(above < depth)
        def _():
            side(above)

    for z in range(depth):
        arrived(z * 4 + second)
        arrived(z * 4 + opposite)

    for z in range(depth):
        index = z * 4 + inner
        send(index, 0, (outer, first, core)).wait_send()
        send(index, 1, (outer, second, core)).wait_send()
        send(z * 4 + first, 1, (outer, second, core)).wait_send()

        @pl.when(jnp.logical_and(outer < depth - 1, z <= outer))
        def _():
            send(index, 2, up).wait_send()

        @pl.when(jnp.logical_and(outer > 0, z >= outer))
        def _():
            send(index, 3, down).wait_send()

    keep.wait()

    @pl.when(core == target_core)
    def _():
        in_keep.wait()

    @pl.when(core != target_core)
    def _():
        in_copy(0).wait_send()

    for offset in range(1, devices):
        in_copy(offset).wait_send()

    def in_wait(index):
        remote(
            in_ref.at[0],
            taken_ref.at[index],
            in_sent.at[0],
            in_landed.at[index],
            (outer, first, core),
        ).wait_recv()

    for lane in range(2):
        for index in range(half):
            local_one = jnp.logical_and(here == core * half + index, core == lane)

            @pl.when(jnp.logical_not(local_one))
            def _():
                in_wait(lane * half + index)

    for which in range(3):
        out_keep(which).wait()
        for offset in range(1, 4):
            out_copy(which, offset).wait_send()
        for offset in range(1, 4):
            other = (inner + offset) % 4
            remote(
                out_from(which, other),
                out_to(which, other),
                out_sent.at[which, 0],
                out_landed.at[which, other],
                (outer, first, core),
            ).wait_recv()


def entry_exchange(own_half, in_block, out_weights, depth):
    devices = 4 * depth
    length, half = own_half.shape
    out_rows, columns = out_weights[0].shape
    any_spec = pl.BlockSpec(memory_space=pl.ANY)
    dma = pltpu.SemaphoreType.DMA
    return pl.pallas_call(
        functools.partial(entry_kernel, depth),
        out_shape=(
            jax.ShapeDtypeStruct((devices * length, half), own_half.dtype),
            jax.ShapeDtypeStruct(in_block.shape, in_block.dtype),
            jax.ShapeDtypeStruct((4 * out_rows, 3 * (columns // 4)), in_block.dtype),
        ),
        in_specs=[any_spec] * 5,
        out_specs=(any_spec,) * 3,
        scratch_shapes=[
            dma((devices, 4)),
            dma((devices,)),
            dma((devices,)),
            dma((devices,)),
            dma((3, 4)),
            dma((3, 4)),
            dma((5,)),
        ],
        compiler_params=pltpu.CompilerParams(has_side_effects=True),
        cost_estimate=pl.CostEstimate(flops=0, bytes_accessed=0, transcendentals=0),
    )(own_half, in_block, *out_weights)


def middle_kernel(depth, mixed_ref, last_ref, turned_ref, states_ref, sent, landed, last_sent, last_landed, local_sem):
    outer, inner, core = (lax.axis_index("outer"), lax.axis_index("inner"), lax.axis_index("tp"))
    devices = 4 * depth
    here = outer * 4 + inner
    keep = pltpu.make_async_copy(mixed_ref.at[here], turned_ref.at[here], local_sem.at[0])
    keep_last = pltpu.make_async_copy(last_ref, states_ref.at[here], local_sem.at[1])
    keep.start()
    keep_last.start()

    def copies(offset):
        other = (here + offset) % devices
        device = (other // 4, other % 4, core)
        return (
            remote(
                mixed_ref.at[other], turned_ref.at[here], sent.at[offset], landed.at[here], device
            ),
            remote(
                last_ref, states_ref.at[here], last_sent.at[offset], last_landed.at[here], device
            ),
        )

    for offset in range(1, devices):
        for copy in copies(offset):
            copy.start()
    keep.wait()
    keep_last.wait()
    for offset in range(1, devices):
        for copy in copies(offset):
            copy.wait_send()
    for offset in range(1, devices):
        other = (here + offset) % devices
        device = (other // 4, other % 4, core)
        remote(
            mixed_ref.at[other], turned_ref.at[other], sent.at[offset], landed.at[other], device
        ).wait_recv()
        remote(
            last_ref, states_ref.at[other], last_sent.at[offset], last_landed.at[other], device
        ).wait_recv()


def middle_exchange(mixed, last, depth):
    devices = 4 * depth
    any_spec = pl.BlockSpec(memory_space=pl.ANY)
    dma = pltpu.SemaphoreType.DMA
    return pl.pallas_call(
        functools.partial(middle_kernel, depth),
        out_shape=(
            jax.ShapeDtypeStruct(mixed.shape, mixed.dtype),
            jax.ShapeDtypeStruct((devices,) + last.shape, last.dtype),
        ),
        in_specs=[any_spec] * 2,
        out_specs=(any_spec,) * 2,
        scratch_shapes=[dma((devices,))] * 4 + [dma((2,))],
        compiler_params=pltpu.CompilerParams(has_side_effects=True),
    )(mixed, last)


def exit_kernel(own_ref, all_ref, sent, landed, local_sem):
    outer, inner, core = (lax.axis_index("outer"), lax.axis_index("inner"), lax.axis_index("tp"))
    first, second, opposite = plane_neighbours(inner, core)
    length, half = own_ref.shape[1:]

    def slot(index, side):
        rows = pl.ds(pl.multiple_of(index * length, length), length)
        return all_ref.at[:, rows, pl.ds(pl.multiple_of(side * half, half), half)]

    def send(index, lane, device, source=None):
        return remote(
            slot(index, core) if source is None else source,
            slot(index, core),
            sent.at[index, lane],
            landed.at[core, index],
            device,
        )

    peer = (outer, inner, 1 - core)
    near, far = ((outer, first, core), (outer, second, core))
    send(inner, 0, near, own_ref).start()
    send(inner, 1, far, own_ref).start()
    send(inner, 2, peer, own_ref).start()
    keep = pltpu.make_async_copy(own_ref, slot(inner, core), local_sem.at[0])
    keep.start()
    send(first, 0, near).wait_recv()
    send(first, 1, far).start()
    send(first, 2, peer).start()
    for index in (second, opposite):
        send(index, 0, near).wait_recv()
        send(index, 2, peer).start()
    for index in range(4):
        remote(
            own_ref,
            slot(index, 1 - core),
            sent.at[index, 2],
            landed.at[1 - core, index],
            peer,
        ).wait_recv()
    send(inner, 0, near).wait_send()
    send(inner, 1, far).wait_send()
    send(first, 1, far).wait_send()
    for index in (inner, first, second, opposite):
        send(index, 2, peer).wait_send()
    keep.wait()


def exit_gather(both):
    parts, length, half = both.shape
    any_spec = pl.BlockSpec(memory_space=pl.ANY)
    dma = pltpu.SemaphoreType.DMA
    return pl.pallas_call(
        exit_kernel,
        out_shape=jax.ShapeDtypeStruct((parts, 4 * length, 2 * half), both.dtype),
        in_specs=[any_spec],
        out_specs=any_spec,
        scratch_shapes=[dma((4, 3)), dma((2, 4)), dma((1,))],
        compiler_params=pltpu.CompilerParams(has_side_effects=True),
    )(both)


def channel_local(
    tokens,
    norm_gain,
    conv_value,
    conv_gate,
    state_feed,
    conv_taps,
    chan_gain,
    chan_shift,
    conv_project,
    decay_rate,
    frequency,
    input_real,
    input_imag,
    output_real,
    output_imag,
    skip_gain,
    state_value,
    state_gate,
    initial_state,
):
    seq = ("outer", "inner")
    devices = lax.axis_size("outer") * lax.axis_size("inner")
    inner = lax.axis_size("inner")
    position = lax.axis_index("outer") * inner + lax.axis_index("inner")
    core = lax.axis_index("tp")
    swap = [(0, 1), (1, 0)]
    local_length, model = tokens.shape
    total = local_length * devices
    half = model // 2
    floats = tokens.astype(jnp.float32)
    normed = (
        floats * lax.rsqrt(jnp.mean(floats * floats, axis=1, keepdims=True) + 1e-06) * norm_gain
    ).astype(jnp.bfloat16)
    own_half = lax.dynamic_slice_in_dim(normed, core * half, half, axis=1)
    rows, wide = conv_value.shape
    share = wide // devices
    in_block = jnp.stack([conv_value, conv_gate, state_feed], axis=1)
    in_block = in_block.reshape(rows, 3, devices, share).transpose(2, 0, 1, 3)
    in_block = in_block.reshape(devices, rows, 3 * share)
    out_rows, columns = conv_project.shape
    piece = columns // inner
    all_half, in_block, out_block = entry_exchange(
        own_half, in_block, (conv_project, state_value, state_gate), lax.axis_size("outer")
    )
    in_block = in_block.reshape(2, half, 3 * share)
    kept = lax.dynamic_index_in_dim(in_block, core, axis=0, keepdims=False)
    taken = lax.dynamic_index_in_dim(in_block, 1 - core, axis=0, keepdims=False)
    out_block = lax.all_gather(out_block, "outer", axis=0, tiled=True)
    groups = decay_rate.shape[0] // devices
    chunk = 8

    def own(value, axis=0, size=groups):
        return lax.dynamic_slice_in_dim(value, position * size, size, axis=axis)

    matrices = chunk_matrices(
        own(decay_rate),
        own(frequency),
        own(input_real),
        own(input_imag),
        own(output_real),
        own(output_imag),
        total,
        chunk,
    )
    other = lax.ppermute(jnp.dot(all_half, taken, preferred_element_type=jnp.float32), "tp", swap)
    projected = jnp.dot(all_half, kept, preferred_element_type=jnp.float32) + other
    gated = (projected[:, :share] * jax.nn.sigmoid(projected[:, share : 2 * share])).astype(
        jnp.bfloat16
    )
    feed = projected[:, 2 * share :].astype(jnp.bfloat16)
    kernel = conv_taps.shape[0]
    taps = own(conv_taps, 1, share)
    padded = jnp.pad(gated, ((kernel - 1, 0), (0, 0))).astype(jnp.float32)
    conv_sum = jnp.zeros((total, share), jnp.float32)
    for offset in range(kernel):
        conv_sum = conv_sum + taps[offset] * padded[offset : offset + total]
    conv_out = conv_sum.astype(jnp.bfloat16)
    start = own(initial_state, 1).reshape(2, -1)
    activated, last = recurrence(feed, own(skip_gain, 0, share), start, matrices, chunk)
    states = initial_state.shape[2]
    mixed = jnp.concatenate([conv_out, activated], axis=1).reshape(devices, local_length, 2 * share)
    mixed, last = middle_exchange(mixed, last.reshape(-1, 128), lax.axis_size("outer"))
    mixed = mixed.transpose(1, 0, 2)
    final_state = last.reshape(devices, 2, groups, states).transpose(1, 0, 2, 3)
    final_state = final_state.reshape(initial_state.shape)
    conv_full = mixed[:, :, :share].reshape(local_length, wide).astype(jnp.float32)
    active = mixed[:, :, share:].reshape(local_length, wide)
    own_mean = jnp.mean(conv_full, axis=1, keepdims=True)
    deviation = conv_full - own_mean
    own_spread = jnp.mean(deviation * deviation, axis=1, keepdims=True)
    peer = lax.ppermute(jnp.concatenate([own_mean, own_spread], axis=1), "tp", swap)
    row_mean = 0.5 * (own_mean + peer[:, :1])
    gap = 0.5 * (own_mean - peer[:, :1])
    variance = 0.5 * (own_spread + peer[:, 1:]) + gap * gap
    gain = lax.dynamic_slice_in_dim(chan_gain, core * wide, wide, axis=0)
    bias = lax.dynamic_slice_in_dim(chan_shift, core * wide, wide, axis=0)
    conv_act = jax.nn.silu(
        (conv_full - row_mean) * lax.rsqrt(variance + 1e-05) * gain + bias
    ).astype(jnp.bfloat16)
    both = jnp.stack([conv_act, active], axis=0)
    both = exit_gather(both)
    conv_branch = jnp.dot(both[0], out_block[:, :piece], preferred_element_type=jnp.float32)
    state_both = jnp.dot(both[1], out_block[:, piece:], preferred_element_type=jnp.float32)
    mixer = (conv_branch + state_both[:, :piece] * jax.nn.sigmoid(state_both[:, piece:])).astype(
        jnp.bfloat16
    )
    mixer = mixer.reshape(inner, local_length, piece)
    mixer = lax.all_to_all(mixer, "inner", 0, 0, tiled=True)
    mixer_out = mixer.transpose(1, 0, 2).reshape(local_length, columns)
    return (mixer_out, final_state)


def specs_of(seq):
    in_specs = (
        P(seq, None),
        P(),
        P(seq, "tp"),
        P(seq, "tp"),
        P(seq, "tp"),
        P(None, "tp"),
        P(),
        P(),
        P(seq, "tp"),
        P("tp", None),
        P("tp", None),
        P("tp", None, None),
        P("tp", None, None),
        P("tp", None, None),
        P("tp", None, None),
        P("tp"),
        P(seq, "tp"),
        P(seq, "tp"),
        P(None, "tp", None),
    )
    return (in_specs, (P(seq, "tp"), P(None, "tp", None)))


def solution(mesh):
    seq_devices, cores = (mesh.shape["sp"], mesh.shape["tp"])
    fine = jax.sharding.Mesh(
        mesh.devices.reshape(seq_devices // 4, 4, cores), ("outer", "inner", "tp")
    )

    def run(*args):
        groups = args[9].shape[0]
        if cores == 2 and groups % (cores * seq_devices) == 0:
            in_specs, out_specs = specs_of(("outer", "inner"))
            body = jax.shard_map(
                channel_local, mesh=fine, in_specs=in_specs, out_specs=out_specs, check_vma=False
            )
        else:
            in_specs, out_specs = specs_of("sp")
            body = jax.shard_map(
                local, mesh=mesh, in_specs=in_specs, out_specs=out_specs, check_vma=False
            )
        return body(*args)

    return run
```

```python
import functools
import jax
import jax.numpy as jnp
from jax import lax
from jax.experimental import pallas as pl
from jax.experimental.pallas import tpu as pltpu
from jax.sharding import PartitionSpec as P


def passed_along(value, axis, steps):
    count = lax.axis_size(axis)
    leading, last = (max(0, -steps), min(count, count - steps))
    return lax.ppermute(value, axis, [(source, source + steps) for source in range(leading, last)])


def rotate(first_real, first_imag, second_real, second_imag):
    return (
        first_real * second_real - first_imag * second_imag,
        first_real * second_imag + first_imag * second_real,
    )


def power_table(base_real, base_imag, exponent, largest):
    result_real = jnp.ones((exponent.shape[0], base_real.shape[0]), jnp.float32)
    result_imag = jnp.zeros((exponent.shape[0], base_real.shape[0]), jnp.float32)
    square_real, square_imag = (base_real, base_imag)
    for place in range(max(largest, 1).bit_length()):
        chosen = (exponent >> place & 1 == 1)[:, None]
        next_real, next_imag = rotate(result_real, result_imag, square_real, square_imag)
        result_real = jnp.where(chosen, next_real, result_real)
        result_imag = jnp.where(chosen, next_imag, result_imag)
        square_real, square_imag = rotate(square_real, square_imag, square_real, square_imag)
    return (result_real, result_imag)


def local(
    tokens,
    norm_gain,
    conv_value,
    conv_gate,
    state_feed,
    conv_taps,
    chan_gain,
    chan_shift,
    conv_project,
    decay_rate,
    frequency,
    input_real,
    input_imag,
    output_real,
    output_imag,
    skip_gain,
    state_value,
    state_gate,
    initial_state,
):
    highest = lax.Precision.HIGHEST
    floats = tokens.astype(jnp.float32)
    normed = (
        floats * lax.rsqrt(jnp.mean(floats * floats, axis=1, keepdims=True) + 1e-06) * norm_gain
    ).astype(jnp.bfloat16)
    length = tokens.shape[0]
    width = conv_value.shape[1]
    in_block = jnp.concatenate([conv_value, conv_gate, state_feed], axis=1)
    projected = jnp.dot(
        normed,
        lax.all_gather(in_block, "sp", axis=0, tiled=True),
        preferred_element_type=jnp.float32,
    )
    gated_linear = (projected[:, :width] * jax.nn.sigmoid(projected[:, width : 2 * width])).astype(
        jnp.bfloat16
    )
    state_drive = projected[:, 2 * width :].astype(jnp.bfloat16)
    kernel = conv_taps.shape[0]
    before = passed_along(gated_linear[length - (kernel - 1) :], "sp", 1)
    padded = jnp.concatenate([before, gated_linear], axis=0).astype(jnp.float32)
    conv_sum = jnp.zeros((length, width), jnp.float32)
    for offset in range(kernel):
        conv_sum = conv_sum + conv_taps[offset] * padded[offset : offset + length]
    conv_out = conv_sum.astype(jnp.bfloat16)
    seq_devices = lax.axis_size("sp")
    total_tokens = length * seq_devices
    groups, state_size, group_size = input_real.shape
    flat = groups * state_size
    rate_real = -decay_rate / total_tokens
    magnitude = jnp.exp(rate_real)
    step_real = magnitude * jnp.cos(frequency)
    step_imag = magnitude * jnp.sin(frequency)
    modulus = rate_real * rate_real + frequency * frequency
    lift_real = step_real - 1.0
    factor_real = (lift_real * rate_real + step_imag * frequency) / modulus
    factor_imag = (step_imag * rate_real - lift_real * frequency) / modulus
    drive_real = factor_real[..., None] * input_real - factor_imag[..., None] * input_imag
    drive_imag = factor_real[..., None] * input_imag + factor_imag[..., None] * input_real
    grouped = state_drive.astype(jnp.float32).reshape(length, groups, group_size)
    pushed_real = jnp.einsum("gph,tgh->tgp", drive_real, grouped, precision=highest).reshape(
        length, flat
    )
    pushed_imag = jnp.einsum("gph,tgh->tgp", drive_imag, grouped, precision=highest).reshape(
        length, flat
    )
    base_real = step_real.reshape(flat)
    base_imag = step_imag.reshape(flat)
    square_size = base_real * base_real + base_imag * base_imag
    back_real = base_real / square_size
    back_imag = -base_imag / square_size
    positions = lax.iota(jnp.int32, length)
    counted = positions + 1
    power_real, power_imag = power_table(base_real, base_imag, counted, length)
    undo_real, undo_imag = power_table(back_real, back_imag, counted, length)
    scaled_real, scaled_imag = rotate(undo_real, undo_imag, pushed_real, pushed_imag)
    lower = (positions[:, None] >= positions[None, :]).astype(jnp.float32)
    summed_real = jnp.dot(lower, scaled_real, precision=highest)
    summed_imag = jnp.dot(lower, scaled_imag, precision=highest)
    local_real, local_imag = rotate(power_real, power_imag, summed_real, summed_imag)
    span_real, span_imag = (power_real[-1], power_imag[-1])
    last_real, last_imag = (local_real[-1], local_imag[-1])
    start_real = initial_state[0].reshape(flat)
    start_imag = initial_state[1].reshape(flat)
    finals = lax.all_gather(jnp.stack([last_real, last_imag])[None], "sp", axis=0, tiled=True)
    position = lax.axis_index("sp")
    device_ids = lax.iota(jnp.int32, seq_devices)
    lag = jnp.maximum(position - 1 - device_ids, 0)
    weight_real, weight_imag = power_table(span_real, span_imag, lag, seq_devices)
    before_mask = (device_ids < position).astype(jnp.float32)[:, None]
    moved_real, moved_imag = rotate(weight_real, weight_imag, finals[:, 0], finals[:, 1])
    lead_real, lead_imag = power_table(
        span_real, span_imag, jnp.stack([position, jnp.int32(seq_devices)]), seq_devices
    )
    opening_real, opening_imag = rotate(lead_real[0], lead_imag[0], start_real, start_imag)
    entry_real = opening_real + jnp.sum(moved_real * before_mask, axis=0)
    entry_imag = opening_imag + jnp.sum(moved_imag * before_mask, axis=0)
    tail_real, tail_imag = power_table(
        span_real, span_imag, seq_devices - 1 - device_ids, seq_devices
    )
    carried_real, carried_imag = rotate(tail_real, tail_imag, finals[:, 0], finals[:, 1])
    closing_real, closing_imag = rotate(lead_real[1], lead_imag[1], start_real, start_imag)
    final_real = closing_real + jnp.sum(carried_real, axis=0)
    final_imag = closing_imag + jnp.sum(carried_imag, axis=0)
    final_state = jnp.stack([final_real, final_imag]).reshape(2, groups, state_size)
    state_real = (power_real * entry_real - power_imag * entry_imag + local_real).reshape(
        length, groups, state_size
    )
    state_imag = (power_real * entry_imag + power_imag * entry_real + local_imag).reshape(
        length, groups, state_size
    )
    response = jnp.einsum("ghp,tgp->tgh", output_real, state_real, precision=highest) - jnp.einsum(
        "ghp,tgp->tgh", output_imag, state_imag, precision=highest
    )
    response = response.reshape(length, groups * group_size) + skip_gain * state_drive.astype(
        jnp.float32
    )
    activated = jax.nn.gelu(response).astype(jnp.bfloat16)
    conv_rows, activated_rows = (
        lax.all_gather(conv_out, "tp", axis=1, tiled=True),
        lax.all_gather(activated, "tp", axis=1, tiled=True),
    )
    conv_full = conv_rows.astype(jnp.float32)
    row_mean = jnp.mean(conv_full, axis=1, keepdims=True)
    centred = conv_full - row_mean
    variance = jnp.mean(centred * centred, axis=1, keepdims=True)
    conv_act = jax.nn.silu(centred * lax.rsqrt(variance + 1e-05) * chan_gain + chan_shift).astype(
        jnp.bfloat16
    )
    columns = conv_project.shape[1]
    out_block = jnp.concatenate([conv_project, state_value, state_gate], axis=1)
    piece = lax.all_gather(out_block, "sp", axis=0, tiled=True)
    conv_branch = jnp.dot(conv_act, piece[:, :columns], preferred_element_type=jnp.float32)
    state_both = jnp.dot(activated_rows, piece[:, columns:], preferred_element_type=jnp.float32)
    mixer_out = (
        conv_branch + state_both[:, :columns] * jax.nn.sigmoid(state_both[:, columns:])
    ).astype(jnp.bfloat16)
    return (mixer_out, final_state)


def power_stack(base_real, base_imag, count):
    real, imag = (base_real[None], base_imag[None])
    while real.shape[0] < count:
        next_real, next_imag = rotate(real, imag, real[-1:], imag[-1:])
        real = jnp.concatenate([real, next_real], axis=0)
        imag = jnp.concatenate([imag, next_imag], axis=0)
    return (real[:count], imag[:count])


def block_diagonal(blocks):
    groups = blocks.shape[1]
    return blocks[:, :, :, None, :] * jnp.eye(groups, dtype=blocks.dtype)[None, :, None, :, None]


def chunk_matrices(decay_rate, frequency, input_real, input_imag, output_real, output_imag, total, chunk):
    highest = lax.Precision.HIGHEST
    groups, states, width = input_real.shape
    rate_real = -decay_rate / total
    magnitude = jnp.exp(rate_real)
    step_real = magnitude * jnp.cos(frequency)
    step_imag = magnitude * jnp.sin(frequency)
    modulus = rate_real * rate_real + frequency * frequency
    lift_real = step_real - 1.0
    factor_real = (lift_real * rate_real + step_imag * frequency) / modulus
    factor_imag = (step_imag * rate_real - lift_real * frequency) / modulus
    drive_real = factor_real[..., None] * input_real - factor_imag[..., None] * input_imag
    drive_imag = factor_real[..., None] * input_imag + factor_imag[..., None] * input_real
    power_real, power_imag = power_stack(step_real, step_imag, chunk)
    whole_real = jnp.concatenate([jnp.ones_like(step_real)[None], power_real], axis=0)
    whole_imag = jnp.concatenate([jnp.zeros_like(step_imag)[None], power_imag], axis=0)
    back_real = whole_real[:chunk][::-1, :, :, None]
    back_imag = whole_imag[:chunk][::-1, :, :, None]
    push_real, push_imag = rotate(back_real, back_imag, drive_real[None], drive_imag[None])
    push = [
        block_diagonal(value.transpose(0, 1, 3, 2)).reshape(chunk * groups * width, groups * states)
        for value in (push_real, push_imag)
    ]
    push = jnp.concatenate(push, axis=1)
    out_real, out_imag = rotate(
        output_real[None], output_imag[None], whole_real[:, :, None, :], whole_imag[:, :, None, :]
    )
    emit = [
        block_diagonal(value.transpose(1, 3, 0, 2).reshape(1, groups, states, chunk * width))
        for value in (out_real[1:], -out_imag[1:])
    ]
    emit = [
        value.reshape(groups, states, groups, chunk, width)
        .transpose(0, 1, 3, 2, 4)
        .reshape(groups * states, chunk * groups * width)
        for value in emit
    ]
    emit = jnp.concatenate(emit, axis=0)
    response = jnp.einsum(
        "dghp,gpi->dgih", out_real[:chunk], drive_real, precision=highest
    ) - jnp.einsum("dghp,gpi->dgih", out_imag[:chunk], drive_imag, precision=highest)
    spread = block_diagonal(response).reshape(chunk, groups * width, groups * width)
    spread = spread.transpose(1, 0, 2).reshape(groups * width, chunk * groups * width)
    padded = jnp.concatenate([jnp.zeros_like(spread), spread], axis=1)
    span = groups * width
    full = chunk * span
    inside = jnp.concatenate(
        [padded[:, full - place * span : 2 * full - place * span] for place in range(chunk)], axis=0
    )
    return (power_real[-1].reshape(-1), power_imag[-1].reshape(-1), push, emit, inside)


def recurrence(feed, skip_gain, start, matrices, chunk):
    highest = lax.Precision.HIGHEST
    span_real, span_imag, push, emit, inside = matrices
    length, width = feed.shape
    count = length // chunk
    rows = feed.reshape(count, chunk * width).astype(jnp.float32)
    pushed = jnp.dot(rows, push, precision=highest)
    flat = span_real.shape[0]
    first_real, first_imag = rotate(span_real, span_imag, start[0], start[1])
    head = jnp.concatenate([first_real, first_imag])[None]
    pushed = jnp.concatenate([pushed[:1] + head, pushed[1:]], axis=0)
    real, imag = (pushed[:, :flat], pushed[:, flat:])
    shift = 1
    while shift < count:
        moved_real = jnp.pad(real[:-shift], ((shift, 0), (0, 0)))
        moved_imag = jnp.pad(imag[:-shift], ((shift, 0), (0, 0)))
        add_real, add_imag = rotate(span_real, span_imag, moved_real, moved_imag)
        real, imag = (real + add_real, imag + add_imag)
        span_real, span_imag = rotate(span_real, span_imag, span_real, span_imag)
        shift *= 2
    entry_real = jnp.concatenate([start[0][None], real[:-1]], axis=0)
    entry_imag = jnp.concatenate([start[1][None], imag[:-1]], axis=0)
    entry = jnp.concatenate([entry_real, entry_imag], axis=1)
    response = jnp.dot(rows, inside, precision=highest) + jnp.dot(entry, emit, precision=highest)
    response = response + jnp.tile(skip_gain, chunk) * rows
    activated = jax.nn.gelu(response).astype(jnp.bfloat16).reshape(length, width)
    return (activated, jnp.stack([real[-1], imag[-1]]))


def remote(source, target, send_sem, recv_sem, device):
    return pltpu.make_async_remote_copy(
        src_ref=source,
        dst_ref=target,
        send_sem=send_sem,
        recv_sem=recv_sem,
        device_id=device,
        device_id_type=pl.DeviceIdType.MESH,
    )


def plane_neighbours(inner, core):
    flip_x = inner + 1 - 2 * (inner % 2)
    flip_y = inner + 2 - 4 * (inner // 2)
    first = flip_x * (1 - core) + flip_y * core
    second = flip_y * (1 - core) + flip_x * core
    return (first, second, 3 - inner)


def entry_kernel(
    depth, own_ref, in_ref, project_ref, value_ref, gate_ref, all_ref, taken_ref, moved_ref, sent,
    landed, in_sent, in_landed, out_sent, out_landed, local_sem
):
    outer, inner, core = (lax.axis_index("outer"), lax.axis_index("inner"), lax.axis_index("tp"))
    first, second, opposite = plane_neighbours(inner, core)
    length = own_ref.shape[0]
    devices = 4 * depth
    here = outer * 4 + inner
    half = devices // 2
    target_core = here // half

    def slot(index):
        return all_ref.at[pl.ds(pl.multiple_of(index * length, length), length)]

    def send(index, lane, device, source=None):
        return remote(
            slot(index) if source is None else source,
            slot(index),
            sent.at[index, lane],
            landed.at[index],
            device,
        )

    def arrived(index):
        send(index, 0, (outer, first, core)).wait_recv()

    def spread(index, source=None):
        send(index, 0, (outer, first, core), source).start()
        send(index, 1, (outer, second, core), source).start()

    up, down = ((outer + 1, inner, core), (outer - 1, inner, core))

    @pl.when(outer < depth - 1)
    def _():
        send(here, 2, up, own_ref).start()

    @pl.when(outer > 0)
    def _():
        send(here, 3, down, own_ref).start()

    spread(here, own_ref)
    keep = pltpu.make_async_copy(own_ref, slot(here), local_sem.at[0])
    keep.start()
    place = core * half + here % half

    def in_copy(offset):
        other = (here + offset) % devices
        return remote(
            in_ref.at[other],
            taken_ref.at[place],
            in_sent.at[offset],
            in_landed.at[place],
            (other // 4, other % 4, target_core),
        )

    in_keep = pltpu.make_async_copy(in_ref.at[here], taken_ref.at[place], local_sem.at[1])

    @pl.when(core == target_core)
    def _():
        in_keep.start()

    @pl.when(core != target_core)
    def _():
        in_copy(0).start()

    for offset in range(1, devices):
        in_copy(offset).start()

    out_refs = (project_ref, value_ref, gate_ref)
    out_rows, columns = project_ref.shape
    piece = columns // 4

    def out_from(which, other):
        return out_refs[which].at[:, pl.ds(pl.multiple_of(other * piece, piece), piece)]

    def out_to(which, origin):
        rows = pl.ds(pl.multiple_of(origin * out_rows, out_rows), out_rows)
        return moved_ref.at[rows, pl.ds(which * piece, piece)]

    def out_keep(which):
        return pltpu.make_async_copy(
            out_from(which, inner), out_to(which, inner), local_sem.at[2 + which]
        )

    def out_copy(which, offset):
        other = (inner + offset) % 4
        return remote(
            out_from(which, other),
            out_to(which, inner),
            out_sent.at[which, offset],
            out_landed.at[which, inner],
            (outer, other, core),
        )

    for which in range(3):
        out_keep(which).start()
        for offset in range(1, 4):
            out_copy(which, offset).start()

    def side(z):
        index = z * 4 + first
        arrived(index)
        send(index, 1, (outer, second, core)).start()

    side(outer)
    for step in range(1, depth):
        below, above = (outer - step, outer + step)

        @pl.when(below >= 0)
        def _():
            index = below * 4 + inner
            arrived(index)

            @pl.when(outer < depth - 1)
            def _():
                send(index, 2, up).start()

            spread(index)

        @pl.when(above < depth)
        def _():
            index = above * 4 + inner
            arrived(index)

            @pl.when(outer > 0)
            def _():
                send(index, 3, down).start()

            spread(index)

        @pl.when(below >= 0)
        def _():
            side(below)

        @pl.when(above < depth)
        def _():
            side(above)

    for z in range(depth):
        arrived(z * 4 + second)
        arrived(z * 4 + opposite)

    for z in range(depth):
        index = z * 4 + inner
        send(index, 0, (outer, first, core)).wait_send()
        send(index, 1, (outer, second, core)).wait_send()
        send(z * 4 + first, 1, (outer, second, core)).wait_send()

        @pl.when(jnp.logical_and(outer < depth - 1, z <= outer))
        def _():
            send(index, 2, up).wait_send()

        @pl.when(jnp.logical_and(outer > 0, z >= outer))
        def _():
            send(index, 3, down).wait_send()

    keep.wait()

    @pl.when(core == target_core)
    def _():
        in_keep.wait()

    @pl.when(core != target_core)
    def _():
        in_copy(0).wait_send()

    for offset in range(1, devices):
        in_copy(offset).wait_send()

    def in_wait(index):
        remote(
            in_ref.at[0],
            taken_ref.at[index],
            in_sent.at[0],
            in_landed.at[index],
            (outer, first, core),
        ).wait_recv()

    for lane in range(2):
        for index in range(half):
            local_one = jnp.logical_and(here == core * half + index, core == lane)

            @pl.when(jnp.logical_not(local_one))
            def _():
                in_wait(lane * half + index)

    for which in range(3):
        out_keep(which).wait()
        for offset in range(1, 4):
            out_copy(which, offset).wait_send()
        for offset in range(1, 4):
            other = (inner + offset) % 4
            remote(
                out_from(which, other),
                out_to(which, other),
                out_sent.at[which, 0],
                out_landed.at[which, other],
                (outer, first, core),
            ).wait_recv()


def entry_exchange(own_half, in_block, out_weights, depth):
    devices = 4 * depth
    length, half = own_half.shape
    out_rows, columns = out_weights[0].shape
    any_spec = pl.BlockSpec(memory_space=pl.ANY)
    dma = pltpu.SemaphoreType.DMA
    return pl.pallas_call(
        functools.partial(entry_kernel, depth),
        out_shape=(
            jax.ShapeDtypeStruct((devices * length, half), own_half.dtype),
            jax.ShapeDtypeStruct(in_block.shape, in_block.dtype),
            jax.ShapeDtypeStruct((4 * out_rows, 3 * (columns // 4)), in_block.dtype),
        ),
        in_specs=[any_spec] * 5,
        out_specs=(any_spec,) * 3,
        scratch_shapes=[
            dma((devices, 4)),
            dma((devices,)),
            dma((devices,)),
            dma((devices,)),
            dma((3, 4)),
            dma((3, 4)),
            dma((5,)),
        ],
        compiler_params=pltpu.CompilerParams(has_side_effects=True),
        cost_estimate=pl.CostEstimate(flops=0, bytes_accessed=0, transcendentals=0),
    )(own_half, in_block, *out_weights)


def middle_kernel(depth, mixed_ref, last_ref, turned_ref, states_ref, sent, landed, last_sent, last_landed, local_sem):
    outer, inner, core = (lax.axis_index("outer"), lax.axis_index("inner"), lax.axis_index("tp"))
    devices = 4 * depth
    here = outer * 4 + inner
    keep = pltpu.make_async_copy(mixed_ref.at[here], turned_ref.at[here], local_sem.at[0])
    keep_last = pltpu.make_async_copy(last_ref, states_ref.at[here], local_sem.at[1])
    keep.start()
    keep_last.start()

    def copies(offset):
        other = (here + offset) % devices
        device = (other // 4, other % 4, core)
        return (
            remote(
                mixed_ref.at[other], turned_ref.at[here], sent.at[offset], landed.at[here], device
            ),
            remote(
                last_ref, states_ref.at[here], last_sent.at[offset], last_landed.at[here], device
            ),
        )

    for offset in range(1, devices):
        for copy in copies(offset):
            copy.start()
    keep.wait()
    keep_last.wait()
    for offset in range(1, devices):
        for copy in copies(offset):
            copy.wait_send()
    for offset in range(1, devices):
        other = (here + offset) % devices
        device = (other // 4, other % 4, core)
        remote(
            mixed_ref.at[other], turned_ref.at[other], sent.at[offset], landed.at[other], device
        ).wait_recv()
        remote(
            last_ref, states_ref.at[other], last_sent.at[offset], last_landed.at[other], device
        ).wait_recv()


def middle_exchange(mixed, last, depth):
    devices = 4 * depth
    any_spec = pl.BlockSpec(memory_space=pl.ANY)
    dma = pltpu.SemaphoreType.DMA
    return pl.pallas_call(
        functools.partial(middle_kernel, depth),
        out_shape=(
            jax.ShapeDtypeStruct(mixed.shape, mixed.dtype),
            jax.ShapeDtypeStruct((devices,) + last.shape, last.dtype),
        ),
        in_specs=[any_spec] * 2,
        out_specs=(any_spec,) * 2,
        scratch_shapes=[dma((devices,))] * 4 + [dma((2,))],
        compiler_params=pltpu.CompilerParams(has_side_effects=True),
    )(mixed, last)


def exit_kernel(own_ref, all_ref, sent, landed, local_sem):
    outer, inner, core = (lax.axis_index("outer"), lax.axis_index("inner"), lax.axis_index("tp"))
    first, second, opposite = plane_neighbours(inner, core)
    length, half = own_ref.shape[1:]

    def slot(index, side):
        rows = pl.ds(pl.multiple_of(index * length, length), length)
        return all_ref.at[:, rows, pl.ds(pl.multiple_of(side * half, half), half)]

    def send(index, lane, device, source=None):
        return remote(
            slot(index, core) if source is None else source,
            slot(index, core),
            sent.at[index, lane],
            landed.at[core, index],
            device,
        )

    peer = (outer, inner, 1 - core)
    near, far = ((outer, first, core), (outer, second, core))
    send(inner, 0, near, own_ref).start()
    send(inner, 1, far, own_ref).start()
    send(inner, 2, peer, own_ref).start()
    keep = pltpu.make_async_copy(own_ref, slot(inner, core), local_sem.at[0])
    keep.start()
    send(first, 0, near).wait_recv()
    send(first, 1, far).start()
    send(first, 2, peer).start()
    for index in (second, opposite):
        send(index, 0, near).wait_recv()
        send(index, 2, peer).start()
    for index in range(4):
        remote(
            own_ref,
            slot(index, 1 - core),
            sent.at[index, 2],
            landed.at[1 - core, index],
            peer,
        ).wait_recv()
    send(inner, 0, near).wait_send()
    send(inner, 1, far).wait_send()
    send(first, 1, far).wait_send()
    for index in (inner, first, second, opposite):
        send(index, 2, peer).wait_send()
    keep.wait()


def exit_gather(both):
    parts, length, half = both.shape
    any_spec = pl.BlockSpec(memory_space=pl.ANY)
    dma = pltpu.SemaphoreType.DMA
    return pl.pallas_call(
        exit_kernel,
        out_shape=jax.ShapeDtypeStruct((parts, 4 * length, 2 * half), both.dtype),
        in_specs=[any_spec],
        out_specs=any_spec,
        scratch_shapes=[dma((4, 3)), dma((2, 4)), dma((1,))],
        compiler_params=pltpu.CompilerParams(has_side_effects=True),
    )(both)


def channel_local(
    tokens,
    norm_gain,
    conv_value,
    conv_gate,
    state_feed,
    conv_taps,
    chan_gain,
    chan_shift,
    conv_project,
    decay_rate,
    frequency,
    input_real,
    input_imag,
    output_real,
    output_imag,
    skip_gain,
    state_value,
    state_gate,
    initial_state,
):
    seq = ("outer", "inner")
    devices = lax.axis_size("outer") * lax.axis_size("inner")
    inner = lax.axis_size("inner")
    position = lax.axis_index("outer") * inner + lax.axis_index("inner")
    core = lax.axis_index("tp")
    swap = [(0, 1), (1, 0)]
    local_length, model = tokens.shape
    total = local_length * devices
    half = model // 2
    floats = tokens.astype(jnp.float32)
    normed = (
        floats * lax.rsqrt(jnp.mean(floats * floats, axis=1, keepdims=True) + 1e-06) * norm_gain
    ).astype(jnp.bfloat16)
    own_half = lax.dynamic_slice_in_dim(normed, core * half, half, axis=1)
    rows, wide = conv_value.shape
    share = wide // devices
    in_block = jnp.concatenate(
        [weight.T.reshape(devices, share, rows) for weight in (conv_value, conv_gate, state_feed)],
        axis=1,
    )
    out_rows, columns = conv_project.shape
    piece = columns // inner
    all_half, in_block, out_block = entry_exchange(
        own_half, in_block, (conv_project, state_value, state_gate), lax.axis_size("outer")
    )
    in_block = in_block.reshape(2, devices // 2, 3 * share, rows).transpose(0, 2, 1, 3)
    in_block = in_block.reshape(6 * share, half)
    out_block = lax.all_gather(out_block, "outer", axis=0, tiled=True)
    groups = decay_rate.shape[0] // devices
    chunk = 8

    def own(value, axis=0, size=groups):
        return lax.dynamic_slice_in_dim(value, position * size, size, axis=axis)

    matrices = chunk_matrices(
        own(decay_rate),
        own(frequency),
        own(input_real),
        own(input_imag),
        own(output_real),
        own(output_imag),
        total,
        chunk,
    )
    partial = lax.dot_general(
        in_block, all_half, (((1,), (1,)), ((), ())), preferred_element_type=jnp.float32
    ).reshape(2, 3 * share, total)
    other = lax.dynamic_index_in_dim(partial, 1 - core, axis=0, keepdims=False)
    kept = lax.dynamic_index_in_dim(partial, core, axis=0, keepdims=False)
    projected = (kept + lax.ppermute(other, "tp", swap)).T
    gated = (projected[:, :share] * jax.nn.sigmoid(projected[:, share : 2 * share])).astype(
        jnp.bfloat16
    )
    feed = projected[:, 2 * share :].astype(jnp.bfloat16)
    kernel = conv_taps.shape[0]
    taps = own(conv_taps, 1, share)
    padded = jnp.pad(gated, ((kernel - 1, 0), (0, 0))).astype(jnp.float32)
    conv_sum = jnp.zeros((total, share), jnp.float32)
    for offset in range(kernel):
        conv_sum = conv_sum + taps[offset] * padded[offset : offset + total]
    conv_out = conv_sum.astype(jnp.bfloat16)
    start = own(initial_state, 1).reshape(2, -1)
    activated, last = recurrence(feed, own(skip_gain, 0, share), start, matrices, chunk)
    states = initial_state.shape[2]
    mixed = jnp.concatenate([conv_out, activated], axis=1).reshape(devices, local_length, 2 * share)
    mixed, last = middle_exchange(mixed, last.reshape(-1, 128), lax.axis_size("outer"))
    mixed = mixed.transpose(1, 0, 2)
    final_state = last.reshape(devices, 2, groups, states).transpose(1, 0, 2, 3)
    final_state = final_state.reshape(initial_state.shape)
    conv_full = mixed[:, :, :share].reshape(local_length, wide).astype(jnp.float32)
    active = mixed[:, :, share:].reshape(local_length, wide)
    own_mean = jnp.mean(conv_full, axis=1, keepdims=True)
    deviation = conv_full - own_mean
    own_spread = jnp.mean(deviation * deviation, axis=1, keepdims=True)
    peer = lax.ppermute(jnp.concatenate([own_mean, own_spread], axis=1), "tp", swap)
    row_mean = 0.5 * (own_mean + peer[:, :1])
    gap = 0.5 * (own_mean - peer[:, :1])
    variance = 0.5 * (own_spread + peer[:, 1:]) + gap * gap
    gain = lax.dynamic_slice_in_dim(chan_gain, core * wide, wide, axis=0)
    bias = lax.dynamic_slice_in_dim(chan_shift, core * wide, wide, axis=0)
    conv_act = jax.nn.silu(
        (conv_full - row_mean) * lax.rsqrt(variance + 1e-05) * gain + bias
    ).astype(jnp.bfloat16)
    both = jnp.stack([conv_act, active], axis=0)
    both = exit_gather(both)
    conv_branch = jnp.dot(both[0], out_block[:, :piece], preferred_element_type=jnp.float32)
    state_both = jnp.dot(both[1], out_block[:, piece:], preferred_element_type=jnp.float32)
    mixer = (conv_branch + state_both[:, :piece] * jax.nn.sigmoid(state_both[:, piece:])).astype(
        jnp.bfloat16
    )
    mixer = mixer.reshape(inner, local_length, piece)
    mixer = lax.all_to_all(mixer, "inner", 0, 0, tiled=True)
    mixer_out = mixer.transpose(1, 0, 2).reshape(local_length, columns)
    return (mixer_out, final_state)


def specs_of(seq):
    in_specs = (
        P(seq, None),
        P(),
        P(seq, "tp"),
        P(seq, "tp"),
        P(seq, "tp"),
        P(None, "tp"),
        P(),
        P(),
        P(seq, "tp"),
        P("tp", None),
        P("tp", None),
        P("tp", None, None),
        P("tp", None, None),
        P("tp", None, None),
        P("tp", None, None),
        P("tp"),
        P(seq, "tp"),
        P(seq, "tp"),
        P(None, "tp", None),
    )
    return (in_specs, (P(seq, "tp"), P(None, "tp", None)))


def solution(mesh):
    seq_devices, cores = (mesh.shape["sp"], mesh.shape["tp"])
    fine = jax.sharding.Mesh(
        mesh.devices.reshape(seq_devices // 4, 4, cores), ("outer", "inner", "tp")
    )

    def run(*args):
        groups = args[9].shape[0]
        if cores == 2 and groups % (cores * seq_devices) == 0:
            in_specs, out_specs = specs_of(("outer", "inner"))
            body = jax.shard_map(
                channel_local, mesh=fine, in_specs=in_specs, out_specs=out_specs, check_vma=False
            )
        else:
            in_specs, out_specs = specs_of("sp")
            body = jax.shard_map(
                local, mesh=mesh, in_specs=in_specs, out_specs=out_specs, check_vma=False
            )
        return body(*args)

    return run
```
